128 devices in a mesh: ep: 32 (over z, y, core), tp: 4 (over x).
Axes of the slice: x: 4, y: 4, z: 4, core: 2. Of those that a mesh axis runs over, the one named last changes fastest.
Arguments:
- hidden: bfloat16 [1024, 2048], P('ep')
- norm_gains: float32 [4, 2048], replicated, may hold values from 0.1 to 1.9
- w_query: bfloat16 [2048, 1024], P(None, 'tp'), may hold values from -0.125 to 0.125
- w_key: bfloat16 [2048, 1024], P(None, 'tp'), may hold values from -0.125 to 0.125
- w_value: bfloat16 [2048, 1024], P(None, 'tp'), may hold values from -0.125 to 0.125
- w_outgate: bfloat16 [2048, 1024], P(None, 'tp'), may hold values from -0.125 to 0.125
- w_input_gate: bfloat16 [2048, 8], replicated, may hold values from -0.125 to 0.125
- w_forget_gate: bfloat16 [2048, 8], replicated, may hold values from -0.125 to 0.125
- forget_bias: float32 [8], replicated, may hold values from -1 to 4
- w_mix_out: bfloat16 [1024, 2048], P('tp')
- state_matrix: float32 [1024, 8, 128, 128], P('ep', 'tp'), may hold values from -0.6 to 0.6
- state_norm: float32 [1024, 8, 128], P('ep', 'tp'), may hold values from -0.6 to 0.6
- state_max: float32 [1024, 8], P('ep', 'tp'), may hold values from -4 to 4
- routes: int32 [1024, 2], P('ep'), may hold values from 0 to 31, all different within a row; in each aligned block of 32 rows (0 to 31, 32 to 63, ...) at most 4 rows name the same one
- route_scores: float32 [1024, 2], P('ep'), may hold values from 0.1 to 1
- expert_gate: bfloat16 [32, 2048, 3584], P('ep', None, 'tp'), may hold values from -0.125 to 0.125
- expert_up: bfloat16 [32, 2048, 3584], P('ep', None, 'tp'), may hold values from -0.125 to 0.125
- expert_down: bfloat16 [32, 3584, 2048], P('ep', 'tp')
- dense_gate: bfloat16 [2048, 5632], P('tp', 'ep'), may hold values from -0.125 to 0.125
- dense_up: bfloat16 [2048, 5632], P('tp', 'ep'), may hold values from -0.125 to 0.125
- dense_down: bfloat16 [5632, 2048], P('ep', 'tp')
- dense_mix: float32 [2048], replicated, may hold values from -0.25 to 0.25
Outputs:
- new_hidden: bfloat16 [1024, 2048], P('ep', 'tp')
- new_matrix: float32 [1024, 8, 128, 128], P('ep', 'tp')
- new_norm: float32 [1024, 8, 128], P('ep', 'tp')
- new_max: float32 [1024, 8], P('ep', 'tp')
The draws below stay inside these ranges and needn't reach their ends.
Inputs may be any that keep to these rules, and one draw needn't show every extreme that they name: `routes`: each row names 2 different experts. Among the rows of one index of ep (an aligned block of 32 rows) no expert is named by more than 4 rows, and in every draw some expert is named by exactly 4 rows of some block.
All inputs are finite; a program needn't handle non-finite values.
Results may differ from the reference program's by a relative error of at most 0.02.
Values may be sent and summed in bfloat16 or wider, within the bound.
A program may use at most 128 MiB of HBM per device.

```python
import math
import jax
import jax.numpy as jnp
import numpy as np
from jax import lax

D = 2048
HEADS = 8
HEAD = 128
FF_E = 3584
FF = 5632
TOP = 2
SEQ_DEV = 32
EXPERTS = 32
CAP = 4
SEQS = 1024
N_EP = 32
N_TP = 4


def column_scaled(key, array_shape, fan_in, marker):
    noise_key, level_key = jax.random.split(jax.random.fold_in(key, marker))
    columns = array_shape[-1]
    position = jnp.arange(columns, dtype=jnp.float32) / columns
    levels = 0.5 * position + 0.5 * jax.random.uniform(level_key, (columns,), jnp.float32)
    noise = jax.random.normal(noise_key, array_shape, jnp.float32)
    scales = 10.0 ** levels
    scales = scales / jnp.sqrt(jnp.mean(scales * scales))
    return (noise * scales * (1.0 / fan_in) ** 0.5).astype(jnp.bfloat16)


def draw_hidden(key, part):
    return column_scaled(key, (SEQS, D), 1, 101)


def draw_w_mix_out(key, part):
    return column_scaled(key, (HEADS * HEAD, D), HEADS * HEAD, 102)


def draw_expert_down(key, part):
    return column_scaled(key, (EXPERTS, FF_E, D), FF_E, 103)


def draw_dense_down(key, part):
    return column_scaled(key, (FF, D), FF, 104)


def block_levels(rng, shape, cuts, low, top_value):
    gain = 1.0
    for axis_at, parts in cuts:
        heights = jax.random.uniform(jax.random.fold_in(jax.random.fold_in(rng, 6), axis_at), (parts,), jnp.float32, low / len(cuts), top_value / len(cuts))
        gain = gain * jnp.repeat(jnp.exp(heights), shape[axis_at] // parts).reshape((-1,) + (1,) * (len(shape) - 1 - axis_at))
    return gain


def deal_out(own_key, own, number, rows, amount, top, limit, lean):
    order = jax.random.permutation(own_key, amount)
    heavy_load, ordinary = load_shares(amount, rows * top, limit, lean, True), load_shares(amount, rows * top, limit, lean, False)
    places = jnp.arange(amount)

    def named(tallies, rotation):
        used = int((tallies > 0).sum())
        fixed = max(1, used // 4)
        passed = fixed + (places - fixed + rotation * (used - fixed)) % max(1, amount - fixed)
        return jnp.zeros((amount,), jnp.int32).at[order[jnp.where(places < fixed, places, passed)]].set(jnp.asarray(tallies, jnp.int32))

    tallies = jnp.where(number % 4 == 0, named(heavy_load, number // 4), named(ordinary, number - number // 4 - 1))
    mixed = jax.random.permutation(jax.random.fold_in(own, 3), amount)
    giver, sink = mixed[0:amount // 2 * 2:2], mixed[1:amount // 2 * 2:2]
    slack = jnp.minimum(tallies[giver] - 1, limit - tallies[sink]) // 2
    slack = jnp.where((giver == order[0]) | (sink == order[0]) | (tallies[sink] == 0), 0, jnp.maximum(slack, 0))
    passed = jax.random.randint(jax.random.fold_in(own, 4), (amount // 2,), 0, 1 << 20) % (slack + 1)
    tallies = tallies.at[giver].add(-passed).at[sink].add(passed)
    members = jnp.searchsorted(jnp.cumsum(tallies), jnp.arange(rows * top), side="right").astype(jnp.int32)
    table = members.reshape(top, rows).T
    table = table[jax.random.permutation(jax.random.fold_in(own, 1), rows)]
    rotation = jax.random.randint(jax.random.fold_in(own, 2), (rows, 1), 0, top)
    return jnp.take_along_axis(table, (jnp.arange(top)[None, :] + rotation) % top, axis=1)


def load_shares(number_of, total, most, lean, full):
    portions = [(1 << 20) // math.isqrt(standing ** lean) + 1 for standing in range(1, number_of + 1)]
    largest = most if full else min(most, max(-(-total // number_of), total * portions[0] // sum(portions)))
    least = 1 if total - largest >= number_of - 1 else 0
    counts, surplus = [largest] + [least] * (number_of - 1), total - largest - least * (number_of - 1)
    while surplus > 0:
        candidates = [i for i in range(1, number_of) if counts[i] < largest] or [i for i in range(1, number_of) if counts[i] < most]
        pool, left = sum([portions[i] for i in candidates]), surplus
        for i in candidates:
            extra = min(most - counts[i], max(1, left * portions[i] // pool), surplus)
            counts[i] = counts[i] + extra
            surplus = surplus - extra
    return np.array(counts)


def normal_values(rng, dims, deviation, reach, shards=(), held_as=jnp.bfloat16):
    values = jax.random.normal(rng, dims, jnp.float32) * deviation
    if len(shards) > 0:
        values = block_levels(rng, dims, shards, -0.22, 0.18) * values
    return jnp.clip(values, min=-reach, max=reach).astype(held_as)


def setup_inputs(seed: int = 0) -> dict:
    arg_keys = jax.random.split(jax.random.key(seed), 23)
    hidden = draw_hidden(jax.random.fold_in(arg_keys[22], 71), 0)
    norm_gains = jnp.clip(1.0 + 0.18 * jax.random.normal(arg_keys[1], (4, D), jnp.float32), 0.1, 1.9)
    w_query = normal_values(arg_keys[2], (D, HEADS * HEAD), D ** -0.5, 0.125, ((1, 4),))
    w_key = normal_values(arg_keys[3], (D, HEADS * HEAD), D ** -0.5, 0.125, ((1, 4),))
    w_value = normal_values(arg_keys[4], (D, HEADS * HEAD), D ** -0.5, 0.125, ((1, 4),))
    w_outgate = normal_values(arg_keys[5], (D, HEADS * HEAD), D ** -0.5, 0.125, ((1, 4),))
    w_input_gate = normal_values(arg_keys[6], (D, HEADS), D ** -0.5, 0.125)
    w_forget_gate = normal_values(arg_keys[7], (D, HEADS), D ** -0.5, 0.125)
    forget_bias = jnp.clip(jax.random.uniform(arg_keys[8], (HEADS,), jnp.float32, -1.0, 4.0), -1.0, 4.0)
    w_mix_out = draw_w_mix_out(jax.random.fold_in(arg_keys[22], 71), 0)
    state_matrix = normal_values(arg_keys[10], (SEQS, HEADS, HEAD, HEAD), 0.1, 0.6, ((0, 32), (1, 4)), jnp.float32)
    state_norm = normal_values(arg_keys[11], (SEQS, HEADS, HEAD), 0.1, 0.6, ((0, 32), (1, 4)), jnp.float32)
    state_max = normal_values(arg_keys[12], (SEQS, HEADS), 1.0, 4.0, ((0, 32), (1, 4)), jnp.float32)
    routes_keys = jax.random.split(jax.random.fold_in(arg_keys[13], 1), SEQS // SEQ_DEV)
    routes_turns = jax.random.permutation(jax.random.fold_in(arg_keys[13], 3), SEQS // SEQ_DEV)
    routes = jax.vmap(lambda own, number: deal_out(jax.random.fold_in(arg_keys[13], 2), own, number, SEQ_DEV, EXPERTS, TOP, CAP, 2))(routes_keys, routes_turns).reshape((SEQS, TOP))
    route_scores = jnp.clip(jnp.exp(math.log(1.0) - 2.3025851 * jax.random.uniform(arg_keys[14], (SEQS, TOP), jnp.float32) ** block_levels(arg_keys[14], (SEQS, TOP), ((0, 32),), -0.2, 0.2)), 0.1, 1.0)
    expert_gate = normal_values(arg_keys[15], (EXPERTS, D, FF_E), D ** -0.5, 0.125, ((0, 32), (2, 4)))
    expert_up = normal_values(arg_keys[16], (EXPERTS, D, FF_E), D ** -0.5, 0.125, ((0, 32), (2, 4)))
    expert_down = draw_expert_down(jax.random.fold_in(arg_keys[22], 71), 0)
    dense_gate = normal_values(arg_keys[18], (D, FF), D ** -0.5, 0.125, ((0, 4), (1, 32)))
    dense_up = normal_values(arg_keys[19], (D, FF), D ** -0.5, 0.125, ((0, 4), (1, 32)))
    dense_down = draw_dense_down(jax.random.fold_in(arg_keys[22], 71), 0)
    dense_mix = normal_values(arg_keys[21], (D,), (D // 4) ** -0.5, 0.25, (), jnp.float32)
    return dict(hidden=hidden, norm_gains=norm_gains, w_query=w_query, w_key=w_key, w_value=w_value, w_outgate=w_outgate, w_input_gate=w_input_gate, w_forget_gate=w_forget_gate, forget_bias=forget_bias, w_mix_out=w_mix_out, state_matrix=state_matrix, state_norm=state_norm, state_max=state_max, routes=routes, route_scores=route_scores, expert_gate=expert_gate, expert_up=expert_up, expert_down=expert_down, dense_gate=dense_gate, dense_up=dense_up, dense_down=dense_down, dense_mix=dense_mix)


EPS = 1e-06

def inverse_rms(values):
    return lax.rsqrt(lax.optimization_barrier(jnp.mean(values * values, axis=-1, keepdims=True)) + EPS)

def settle(values):
    return lax.optimization_barrier(values.astype(jnp.bfloat16)).astype(jnp.float32)

def grouped_product(activations, weights_in):
    row_count, inner_width = activations.shape
    group_width = inner_width // N_TP
    left_side = activations.astype(jnp.float32).reshape(row_count, N_TP, group_width)
    right_side = weights_in.astype(jnp.float32).reshape(N_TP, group_width, weights_in.shape[1])
    pieces = settle(jnp.einsum('rbf,bfd->brd', left_side, right_side))
    return lax.optimization_barrier(jnp.sum(pieces, axis=0)).astype(jnp.bfloat16)

def reference(hidden, norm_gains, w_query, w_key, w_value, w_outgate, w_input_gate, w_forget_gate, forget_bias, w_mix_out, state_matrix, state_norm, state_max, routes, route_scores, expert_gate, expert_up, expert_down, dense_gate, dense_up, dense_down, dense_mix):
    start_f = hidden.astype(jnp.float32)
    normed_in = (start_f * inverse_rms(start_f) * norm_gains[0]).astype(jnp.bfloat16)

    def project(weight):
        return settle(jnp.dot(normed_in, weight, preferred_element_type=jnp.float32))
    query = project(w_query).reshape(SEQS, HEADS, HEAD)
    keys = project(w_key).reshape(SEQS, HEADS, HEAD) * HEAD ** (-0.5)
    values = project(w_value).reshape(SEQS, HEADS, HEAD)
    out_gate = project(w_outgate)
    in_gate = jnp.dot(normed_in, w_input_gate, preferred_element_type=jnp.float32)
    log_forget = jax.nn.log_sigmoid(jnp.dot(normed_in, w_forget_gate, preferred_element_type=jnp.float32) + forget_bias)
    carried = log_forget + state_max
    new_max = jnp.maximum(carried, in_gate)
    keep = jnp.exp(carried - new_max)
    write = jnp.exp(in_gate - new_max)
    written = write[:, :, None] * keys
    new_matrix = keep[:, :, None, None] * state_matrix + written[:, :, :, None] * values[:, :, None, :]
    new_norm = keep[:, :, None] * state_norm + written
    numer = jnp.einsum('shd,shdv->shv', query, new_matrix)
    denom = jnp.einsum('shd,shd->sh', query, new_norm)
    read = numer / jnp.maximum(jnp.abs(denom), jnp.exp(-new_max))[:, :, None]
    mixed = (jax.nn.sigmoid(out_gate) * read.reshape(SEQS, HEADS * HEAD)).astype(jnp.bfloat16)
    branch = settle(grouped_product(mixed, w_mix_out))
    residual_f = start_f + norm_gains[1] * branch * inverse_rms(branch)
    residual = settle(residual_f)
    scale_two = inverse_rms(residual_f)
    normed = (residual_f * scale_two * norm_gains[2]).astype(jnp.bfloat16)
    mix_gate = jax.nn.sigmoid(scale_two[:, 0] * lax.optimization_barrier(jnp.sum(residual_f * norm_gains[2] * dense_mix, axis=-1)))
    dense_pre_gate = jnp.dot(normed, dense_gate, preferred_element_type=jnp.float32)
    dense_pre_up = jnp.dot(normed, dense_up, preferred_element_type=jnp.float32)
    dense_hidden = (jax.nn.silu(dense_pre_gate) * dense_pre_up).astype(jnp.bfloat16)
    dense_out = jnp.dot(dense_hidden, dense_down, preferred_element_type=jnp.float32)
    pairs = routes.reshape(N_EP, SEQ_DEV * TOP).astype(jnp.int32)
    picks = (pairs[:, :, None] == jnp.arange(EXPERTS, dtype=jnp.int32)[None, None, :]).astype(jnp.int32)
    ranks = (lax.optimization_barrier(jnp.sum(jnp.cumsum(picks, axis=1) * picks, axis=-1)) - 1).astype(jnp.int32)
    buffer_row = (jnp.arange(N_EP, dtype=jnp.int32)[:, None] * CAP + ranks).reshape(-1).astype(jnp.int32)
    flat_expert = pairs.reshape(-1)
    token_index = (jnp.arange(SEQS * TOP, dtype=jnp.int32) // TOP).astype(jnp.int32)
    expert_in = jnp.zeros((EXPERTS, N_EP * CAP, D), jnp.bfloat16).at[flat_expert, buffer_row].set(normed[token_index])

    def run_expert(operands):
        inputs, gate_weight, up_weight, down_weight = operands
        gate_pre = jnp.dot(inputs, gate_weight, preferred_element_type=jnp.float32)
        up_pre = jnp.dot(inputs, up_weight, preferred_element_type=jnp.float32)
        hidden_units = (jax.nn.silu(gate_pre) * up_pre).astype(jnp.bfloat16)
        return grouped_product(hidden_units, down_weight)
    expert_out = lax.map(run_expert, (expert_in, expert_gate, expert_up, expert_down))
    picked = settle(expert_out[flat_expert, buffer_row]).reshape(SEQS, TOP, D)
    share = route_scores / lax.optimization_barrier(jnp.sum(route_scores, axis=-1, keepdims=True))
    ffn = lax.optimization_barrier(jnp.sum(share[:, :, None] * picked, axis=1)) + mix_gate[:, None] * dense_out
    new_hidden = (residual + norm_gains[3] * ffn * inverse_rms(ffn)).astype(jnp.bfloat16)
    return (new_hidden, new_matrix, new_norm, new_max)
```

```python
import functools

import jax
import jax.numpy as jnp
from jax import lax
from jax.experimental import pallas as pl
from jax.experimental.pallas import tpu as pltpu
from jax.sharding import PartitionSpec as P

EPS = 1e-06
MESH = pl.DeviceIdType.MESH
BF = jnp.bfloat16
F32 = jnp.float32
I32 = jnp.int32
CH = 512


def dot(a, b):
    return jnp.dot(a, b, preferred_element_type=F32)


def iota(shape, dim):
    return lax.broadcasted_iota(I32, shape, dim)


def one_hot(columns, rows, target):
    return (iota((rows, columns), 1) == target(iota((rows, columns), 0))).astype(BF)


def stacked(ref):
    return jnp.concatenate([ref[:, q * CH : (q + 1) * CH] for q in range(4)], axis=0)


def row_total(values):
    part = jnp.sum(values, axis=1, keepdims=True)
    total = part[0:8] + part[8:16] + part[16:24] + part[24:32]
    return jnp.concatenate([total] * 4, axis=0)


def silu(t):
    return t / (1.0 + jnp.exp(-t))


def rest_kernel(
    terms, hidden, gains, mix, routes, scores, eg, eu, ed, dg, du, dd,
    out,
    wg, wu, wd, dgv, duv, gbuf, dbuf,
    bsend, brecv, hperm, nall, tok, osend, orecv, rsend, rrecv, dsend, drecv,
    msend, mrecv, fsend, frecv,
    pm, pmi, pd, pdi, gk, xs, xd, ys, yd, hexp, hden, resid_s, mixg_s, share_s,
    load_sem, b_sem, n_sem, t_sem, o_sem, r_sem, d_sem, m_sem, f_sem,
    gs_sem, gr_sem, ds_sem, dr_sem,
):
    x = lax.axis_index("tp")
    ep = lax.axis_index("ep")
    c = ep % 2
    y = (ep // 2) % 4
    z = ep // 8
    p = ep // 2
    mate = p * 2 + (1 - c)
    left, right, far = (x + 3) % 4, (x + 1) % 4, (x + 2) % 4

    def plane(k):
        return ((z + k // 8) % 4) * 8 + ((y + (k // 2) % 4) % 4) * 2 + (c + k % 2) % 2

    def remote(src, dst, ssem, rsem, to_ep, to_x):
        return pltpu.make_async_remote_copy(
            src_ref=src, dst_ref=dst, send_sem=ssem, recv_sem=rsem,
            device_id=(to_ep, to_x), device_id_type=MESH,
        )

    def landed(ref, sem):
        pltpu.make_async_copy(ref, ref, sem).wait()

    barrier = pltpu.get_barrier_semaphore()

    def greet(k, carry):
        pl.semaphore_signal(barrier, inc=1, device_id=(plane(k), x), device_id_type=MESH)
        return carry

    for d in (2, 1, 3):
        pl.semaphore_signal(barrier, inc=1, device_id=(ep, (x + d) % 4), device_id_type=MESH)
    lax.fori_loop(1, 32, greet, 0)

    loads = [
        pltpu.make_async_copy(src, dst, load_sem.at[n])
        for n, (src, dst) in enumerate(
            [(dg, dgv), (du, duv), (dd, dbuf.at[c, x]), (eg, wg), (eu, wu), (ed, wd)]
        )
    ]
    for load in loads:
        load.start()

    order = one_hot(128, 128, lambda r: ((r >> 3) & 3) * 32 + (r >> 5) * 8 + (r & 7))
    bsend[...] = dot(order, stacked(terms)).astype(BF).reshape(4, 32, CH)
    brecv[x] = bsend[x]
    pl.semaphore_wait(barrier, 34)
    branch_out = []
    for d in (2, 1, 3):
        to = (x + d) % 4
        branch_out.append(remote(bsend.at[to], brecv.at[x], b_sem.at[0], b_sem.at[1], ep, to))
        branch_out[-1].start()

    hperm[...] = dot(order, stacked(hidden)).reshape(4, 32, CH)

    expert0, expert1 = routes[:, 0:1], routes[:, 1:2]
    lane32 = iota((32, 32), 1)
    hot0 = (lane32 == expert0).astype(F32)
    hot1 = (lane32 == expert1).astype(F32)
    earlier = (iota((32, 32), 0) > lane32).astype(BF)
    before = dot(earlier, (hot0 + hot1).astype(BF))
    score0, score1 = scores[:, 0:1], scores[:, 1:2]
    whole = score0 + score1

    def by_piece(column, step):
        return jnp.concatenate(
            [column[xx * 8 : xx * 8 + 8] + q * step for xx in range(4) for q in range(4)], axis=0
        )

    for k, (expert, hot, score) in enumerate(((expert0, hot0, score0), (expert1, hot1, score1))):
        rank = jnp.sum(hot * before, axis=1, keepdims=True).astype(I32)
        place = by_piece(expert * 16 + rank, 4)
        gk[k] = (iota((128, 512), 1) == place).astype(BF)
        share_s[k] = jnp.broadcast_to(by_piece(score / whole, 0.0), (128, 128))
    pm[...] = one_hot(512, 512, lambda r: ((r >> 2) & 31) * 16 + (r >> 7) * 4 + (r & 3))
    pmi[...] = one_hot(512, 512, lambda r: ((r >> 2) & 3) * 128 + (r >> 4) * 4 + (r & 3))
    pd[...] = one_hot(512, 512, lambda r: ((r >> 3) & 15) * 32 + (r >> 7) * 8 + (r & 7))
    pdi[...] = one_hot(512, 512, lambda r: ((r >> 3) & 3) * 128 + (r >> 5) * 8 + (r & 7))

    def gain(k):
        return jnp.concatenate(
            [jnp.broadcast_to(gains[k : k + 1, q * CH : (q + 1) * CH], (8, CH)) for q in range(4)],
            axis=0,
        )

    mix_rows = jnp.concatenate(
        [jnp.broadcast_to(mix[0:1, q * CH : (q + 1) * CH], (8, CH)) for q in range(4)], axis=0
    )

    landed(brecv.at[pl.ds(0, 3)], b_sem.at[1])
    branch = brecv[0].astype(F32) + brecv[1].astype(F32) + brecv[2].astype(F32) + brecv[3].astype(F32)
    branch = branch.astype(BF).astype(F32)
    residual_f = hperm[x] + gain(1) * branch * lax.rsqrt(row_total(branch * branch) / 2048.0 + EPS)
    scale_two = lax.rsqrt(row_total(residual_f * residual_f) / 2048.0 + EPS)
    normed = (residual_f * scale_two * gain(2)).astype(BF)
    nall[x] = normed
    tok[p] = normed

    token_out = []
    for d in (2, 1, 3):
        to = (x + d) % 4
        token_out.append(remote(nall.at[x], nall.at[x], n_sem.at[0], n_sem.at[1], ep, to))
        token_out[-1].start()

    def share_tokens(k, carry):
        to = ((z + k // 4) % 4) * 8 + ((y + k % 4) % 4) * 2 + c
        remote(nall.at[x], tok.at[p], t_sem.at[0], t_sem.at[1], to, x).start()
        return carry

    resid_s[...] = residual_f.astype(BF).astype(F32)
    mix_dot = scale_two * row_total(residual_f * gain(2) * mix_rows)
    mixg_s[...] = jnp.broadcast_to(1.0 / (1.0 + jnp.exp(-mix_dot)), (32, 128))

    landed(nall.at[pl.ds(0, 3)], n_sem.at[1])
    chosen = gk[0] + gk[1]
    rows = lax.dot_general(
        chosen, nall[...].reshape(128, CH), (((0,), (0,)), ((), ())), preferred_element_type=F32
    )
    osend[...] = rows.astype(BF).reshape(32, 16, CH)
    orecv[ep] = osend[ep]

    def dispatch(k, carry):
        to = plane(k)
        remote(osend.at[to], orecv.at[ep], o_sem.at[0], o_sem.at[1], to, x).start()
        return carry

    lax.fori_loop(1, 32, dispatch, 0)
    lax.fori_loop(1, 16, share_tokens, 0)

    loads[0].wait()
    loads[1].wait()
    r176, l384 = iota((176, 384), 0), iota((176, 384), 1)
    into_gate = (l384 == jnp.where(r176 < 128, r176, r176 + 128)).astype(BF)
    into_up = (l384 == jnp.where(r176 < 128, r176 + 128, r176 + 192)).astype(BF)
    gbuf[c, x] = (dot(dgv[...], into_gate) + dot(duv[...], into_up)).astype(BF)
    loads[2].wait()

    def first_round(buf, ssem, rsem):
        block = buf.at[c, x]
        copies = [
            remote(block, block, ssem.at[0], rsem.at[0], ep, right),
            remote(block, block, ssem.at[1], rsem.at[1], ep, left),
            remote(block, block, ssem.at[4], rsem.at[4], mate, x),
        ]
        for copy in copies:
            copy.start()
        return copies

    def second_round(buf, cut, ssem, rsem):
        size = buf.shape[2]
        from_left, from_right = buf.at[c, left], buf.at[c, right]
        low = buf.at[c, left, pl.ds(0, cut)]
        high = buf.at[c, right, pl.ds(cut, size - cut)]
        copies = [
            remote(low, low, ssem.at[2], rsem.at[2], ep, right),
            remote(from_left, from_left, ssem.at[5], rsem.at[5], mate, x),
            remote(high, high, ssem.at[3], rsem.at[3], ep, left),
            remote(from_right, from_right, ssem.at[6], rsem.at[6], mate, x),
        ]
        landed(from_left, rsem.at[0])
        copies[0].start()
        copies[1].start()
        landed(from_right, rsem.at[1])
        copies[2].start()
        copies[3].start()
        return copies

    def third_round(buf, cut, ssem, rsem):
        size = buf.shape[2]
        block = buf.at[c, far]
        landed(buf.at[c, far, pl.ds(0, cut)], rsem.at[2])
        landed(buf.at[c, far, pl.ds(cut, size - cut)], rsem.at[3])
        copy = remote(block, block, ssem.at[7], rsem.at[7], mate, x)
        copy.start()
        return [copy]

    def from_mate(buf, rsem):
        for n, place in ((4, x), (5, left), (6, right), (7, far)):
            landed(buf.at[1 - c, place], rsem.at[n])

    weight_out = first_round(gbuf, gs_sem, gr_sem) + first_round(dbuf, ds_sem, dr_sem)
    weight_out += second_round(gbuf, 256, gs_sem, gr_sem)

    landed(orecv.at[pl.ds(0, 31)], o_sem.at[1])
    xs[...] = dot(pm[...], orecv[...].reshape(512, CH)).astype(BF).reshape(4, 128, CH)
    loads[3].wait()
    loads[4].wait()
    gate_pre = dot(xs[0], wg[0])
    up_pre = dot(xs[0], wu[0])
    for q in range(1, 4):
        gate_pre += dot(xs[q], wg[q])
        up_pre += dot(xs[q], wu[q])
    hexp[...] = (silu(gate_pre) * up_pre).astype(BF)
    loads[5].wait()
    for q in range(4):
        ys[q * 128 : (q + 1) * 128] = dot(hexp[...], wd[:, q * CH : (q + 1) * CH]).astype(BF)
    rsend[...] = dot(pmi[...], ys[...]).astype(BF).reshape(32, 16, CH)
    rrecv[ep] = rsend[ep]

    def give_back(k, carry):
        to = plane(k)
        remote(rsend.at[to], rrecv.at[ep], r_sem.at[0], r_sem.at[1], to, x).start()
        return carry

    lax.fori_loop(1, 32, give_back, 0)

    weight_out += third_round(gbuf, 256, gs_sem, gr_sem)
    weight_out += second_round(dbuf, 96, ds_sem, dr_sem)

    landed(tok.at[pl.ds(0, 15)], t_sem.at[1])
    xd[...] = dot(pd[...], tok[...].reshape(512, CH)).astype(BF).reshape(4, 128, CH)
    from_mate(gbuf, gr_sem)
    for core in range(2):
        pre = dot(xd[0], gbuf[core, 0])
        for q in range(1, 4):
            pre += dot(xd[q], gbuf[core, q])
        tail = pre[:, 256:384]
        hden[core, :, 0:128] = (silu(pre[:, 0:128]) * pre[:, 128:256]).astype(BF)
        hden[core, :, 128:256] = (silu(tail) * pltpu.roll(tail, 64, 1)).astype(BF)
    weight_out += third_round(dbuf, 96, ds_sem, dr_sem)
    from_mate(dbuf, dr_sem)
    for q in range(4):
        yd[q * 128 : (q + 1) * 128] = (
            dot(hden[0, :, 0:176], dbuf[0, q]) + dot(hden[1, :, 0:176], dbuf[1, q])
        ).astype(BF)
    dsend[...] = dot(pdi[...], yd[...]).astype(BF).reshape(16, 32, CH)
    drecv[p] = dsend[p]

    def dense_back(k, carry):
        to = ((z + k // 4) % 4) * 4 + (y + k % 4) % 4
        remote(dsend.at[to], drecv.at[p], d_sem.at[0], d_sem.at[1], to * 2 + c, x).start()
        return carry

    lax.fori_loop(1, 16, dense_back, 0)

    landed(rrecv.at[pl.ds(0, 31)], r_sem.at[1])
    back = rrecv[...].reshape(512, CH)
    moe = share_s[0][:, 0:1] * dot(gk[0], back) + share_s[1][:, 0:1] * dot(gk[1], back)
    msend[...] = moe.astype(BF).reshape(4, 32, CH)
    mrecv[x] = msend[x]
    moe_out = []
    for d in (2, 1, 3):
        to = (x + d) % 4
        moe_out.append(remote(msend.at[to], mrecv.at[x], m_sem.at[0], m_sem.at[1], ep, to))
        moe_out[-1].start()

    landed(drecv.at[pl.ds(0, 15)], d_sem.at[1])
    dense = drecv[0].astype(F32)
    for n in range(1, 16):
        dense += drecv[n].astype(F32)
    landed(mrecv.at[pl.ds(0, 3)], m_sem.at[1])
    ffn = mrecv[0].astype(F32) + mrecv[1].astype(F32) + mrecv[2].astype(F32) + mrecv[3].astype(F32)
    ffn += mixg_s[:, 0:1] * dense
    scale_ffn = lax.rsqrt(row_total(ffn * ffn) / 2048.0 + EPS)
    fsend[...] = (resid_s[...] + gain(3) * ffn * scale_ffn).reshape(4, 8, CH)
    frecv[x] = fsend[x]
    last_out = []
    for d in (2, 1, 3):
        to = (x + d) % 4
        last_out.append(remote(fsend.at[to], frecv.at[x], f_sem.at[0], f_sem.at[1], ep, to))
        last_out[-1].start()

    for copy in weight_out:
        copy.wait_send()
    landed(bsend.at[pl.ds(0, 3)], b_sem.at[0])
    landed(nall.at[pl.ds(0, 3)], n_sem.at[0])
    landed(tok.at[pl.ds(0, 15)], t_sem.at[0])
    landed(osend.at[pl.ds(0, 31)], o_sem.at[0])
    landed(rsend.at[pl.ds(0, 31)], r_sem.at[0])
    landed(dsend.at[pl.ds(0, 15)], d_sem.at[0])
    landed(msend.at[pl.ds(0, 3)], m_sem.at[0])
    landed(frecv.at[pl.ds(0, 3)], f_sem.at[1])
    out[...] = frecv[...].reshape(32, CH).astype(BF)
    landed(fsend.at[pl.ds(0, 3)], f_sem.at[0])


def rest(terms, hidden, gains, mix, routes, scores, eg, eu, ed, dg, du, dd):
    V = pltpu.VMEM
    dma = pltpu.SemaphoreType.DMA
    vm = pl.BlockSpec(memory_space=pltpu.VMEM)
    hb = pl.BlockSpec(memory_space=pl.ANY)
    return pl.pallas_call(
        rest_kernel,
        out_shape=jax.ShapeDtypeStruct((32, CH), BF),
        in_specs=[vm] * 6 + [hb] * 6,
        out_specs=vm,
        scratch_shapes=[
            V((4, 512, 896), BF), V((4, 512, 896), BF), V((896, 2048), BF),
            V((512, 176), BF), V((512, 176), BF), V((2, 4, 512, 384), BF), V((2, 4, 176, 512), BF),
            V((4, 32, CH), BF), V((4, 32, CH), BF), V((4, 32, CH), F32), V((4, 32, CH), BF),
            V((16, 32, CH), BF),
            V((32, 16, CH), BF), V((32, 16, CH), BF), V((32, 16, CH), BF), V((32, 16, CH), BF),
            V((16, 32, CH), BF), V((16, 32, CH), BF),
            V((4, 32, CH), BF), V((4, 32, CH), BF), V((4, 8, CH), F32), V((4, 8, CH), F32),
            V((512, 512), BF), V((512, 512), BF), V((512, 512), BF), V((512, 512), BF),
            V((2, 128, 512), BF), V((4, 128, CH), BF), V((4, 128, CH), BF),
            V((512, CH), BF), V((512, CH), BF), V((128, 896), BF), V((2, 128, 256), BF),
            V((32, CH), F32), V((32, 128), F32), V((2, 128, 128), F32),
            dma((6,)), dma((2,)), dma((2,)), dma((2,)), dma((2,)), dma((2,)), dma((2,)),
            dma((2,)), dma((2,)), dma((8,)), dma((8,)), dma((8,)), dma((8,)),
        ],
        compiler_params=pltpu.CompilerParams(
            collective_id=0, has_side_effects=True, vmem_limit_bytes=60 * 1024 * 1024
        ),
        name="rest",
    )(terms, hidden, gains, mix, routes, scores, eg, eu, ed, dg, du, dd)


def settle(values):
    return lax.optimization_barrier(values.astype(jnp.bfloat16)).astype(jnp.float32)


def local(
    hidden,
    norm_gains,
    w_query,
    w_key,
    w_value,
    w_outgate,
    w_input_gate,
    w_forget_gate,
    forget_bias,
    w_mix_out,
    state_matrix,
    state_norm,
    state_max,
    routes,
    route_scores,
    expert_gate,
    expert_up,
    expert_down,
    dense_gate,
    dense_up,
    dense_down,
    dense_mix,
):
    tp_place = lax.axis_index("tp")
    seq_local, width = hidden.shape
    heads_local = state_matrix.shape[1]
    head_width = state_matrix.shape[2]
    start_f = hidden.astype(jnp.float32)
    normed_in = (
        start_f
        * lax.rsqrt(jnp.mean(start_f * start_f, axis=-1, keepdims=True) + EPS)
        * norm_gains[0]
    ).astype(jnp.bfloat16)
    query_f = jnp.dot(normed_in, w_query, preferred_element_type=jnp.float32)
    key_f = jnp.dot(normed_in, w_key, preferred_element_type=jnp.float32)
    value_f = jnp.dot(normed_in, w_value, preferred_element_type=jnp.float32)
    gate_f = jnp.dot(normed_in, w_outgate, preferred_element_type=jnp.float32)
    head_first = tp_place * heads_local
    input_weight = lax.dynamic_slice_in_dim(w_input_gate, head_first, heads_local, 1)
    forget_weight = lax.dynamic_slice_in_dim(w_forget_gate, head_first, heads_local, 1)
    forget_local = lax.dynamic_slice_in_dim(forget_bias, head_first, heads_local, 0)
    in_gate = jnp.dot(normed_in, input_weight, preferred_element_type=jnp.float32)
    log_forget = jax.nn.log_sigmoid(
        jnp.dot(normed_in, forget_weight, preferred_element_type=jnp.float32) + forget_local
    )
    query = settle(query_f).reshape(seq_local, heads_local, head_width)
    keys = settle(key_f).reshape(seq_local, heads_local, head_width) * head_width ** (-0.5)
    values = settle(value_f).reshape(seq_local, heads_local, head_width)
    carried = log_forget + state_max
    new_max = jnp.maximum(carried, in_gate)
    keep = jnp.exp(carried - new_max)
    write = jnp.exp(in_gate - new_max)
    written = write[:, :, None] * keys
    new_matrix = (
        keep[:, :, None, None] * state_matrix + written[:, :, :, None] * values[:, :, None, :]
    )
    new_norm = keep[:, :, None] * state_norm + written
    numer = jnp.einsum("shd,shdv->shv", query, new_matrix)
    denom = jnp.einsum("shd,shd->sh", query, new_norm)
    read = numer / jnp.maximum(jnp.abs(denom), jnp.exp(-new_max))[:, :, None]
    mixed = (
        jax.nn.sigmoid(settle(gate_f)) * read.reshape(seq_local, heads_local * head_width)
    ).astype(jnp.bfloat16)
    branch_terms = settle(jnp.dot(mixed, w_mix_out, preferred_element_type=jnp.float32))
    new_hidden = rest(
        branch_terms.astype(jnp.bfloat16),
        hidden,
        norm_gains,
        dense_mix.reshape(1, -1),
        routes,
        route_scores,
        expert_gate.reshape(4, CH, -1),
        expert_up.reshape(4, CH, -1),
        expert_down[0],
        dense_gate,
        dense_up,
        dense_down,
    )
    return (new_hidden, new_matrix, new_norm, new_max)


def solution(mesh):
    placed = (
        P("ep", None),
        P(),
        P(None, "tp"),
        P(None, "tp"),
        P(None, "tp"),
        P(None, "tp"),
        P(),
        P(),
        P(),
        P("tp", None),
        P("ep", "tp", None, None),
        P("ep", "tp", None),
        P("ep", "tp"),
        P("ep", None),
        P("ep", None),
        P("ep", None, "tp"),
        P("ep", None, "tp"),
        P("ep", "tp", None),
        P("tp", "ep"),
        P("tp", "ep"),
        P("ep", "tp"),
        P(),
    )
    return jax.shard_map(
        local,
        mesh=mesh,
        in_specs=placed,
        out_specs=(P("ep", "tp"), P("ep", "tp", None, None), P("ep", "tp", None), P("ep", "tp")),
        check_vma=False,
    )
```

```python
import jax
import jax.numpy as jnp
from jax import lax
from jax.experimental import pallas as pl
from jax.experimental.pallas import tpu as pltpu
from jax.sharding import PartitionSpec as P

EPS = 1e-06
MESH = pl.DeviceIdType.MESH
BF = jnp.bfloat16
F32 = jnp.float32
I32 = jnp.int32
CH = 512


def dot(a, b):
    return jnp.dot(a, b, preferred_element_type=F32)


def iota(shape, dim):
    return lax.broadcasted_iota(I32, shape, dim)


def one_hot(columns, rows, target):
    return (iota((rows, columns), 1) == target(iota((rows, columns), 0))).astype(BF)


def stacked(ref):
    return jnp.concatenate([ref[:, q * CH : (q + 1) * CH] for q in range(4)], axis=0)


def row_total(values):
    part = jnp.sum(values, axis=1, keepdims=True)
    total = part[0:8] + part[8:16] + part[16:24] + part[24:32]
    return jnp.concatenate([total] * 4, axis=0)


def silu(t):
    return t / (1.0 + jnp.exp(-t))


def whole_kernel(
    hidden, gains, mix, routes, scores, w_in, w_fg, bias, smax, snorm,
    wq_h, wk_h, wv_h, wo_h, wm_h, st_h, eg, eu, ed, dg, du, dd,
    out, keep_out, written_out, value_out, norm_out, max_out,
    wq, wk, wv, wo, wm, st, numer,
    wg, wu, wd, gbuf, ubuf, dbuf,
    bsend, brecv, hperm, nall, tok, osend, orecv, rsend, rrecv, dsend, drecv,
    msend, mrecv, fsend, frecv,
    pm, pmi, pd, pdi, gk, xs, xd, ys, yd, hexp, hden, resid_s, mixg_s, share_s,
    load_sem, b_sem, n_sem, t_sem, o_sem, r_sem, d_sem, m_sem, f_sem,
    gs_sem, gr_sem, us_sem, ur_sem, ds_sem, dr_sem,
):
    x = lax.axis_index("tp")
    ep = lax.axis_index("ep")
    c = ep % 2
    y = (ep // 2) % 4
    z = ep // 8
    p = ep // 2
    mate = p * 2 + (1 - c)
    left, right, far = (x + 3) % 4, (x + 1) % 4, (x + 2) % 4

    def plane(k):
        return ((z + k // 8) % 4) * 8 + ((y + (k // 2) % 4) % 4) * 2 + (c + k % 2) % 2

    def remote(src, dst, ssem, rsem, to_ep, to_x):
        return pltpu.make_async_remote_copy(
            src_ref=src, dst_ref=dst, send_sem=ssem, recv_sem=rsem,
            device_id=(to_ep, to_x), device_id_type=MESH,
        )

    def landed(ref, sem):
        pltpu.make_async_copy(ref, ref, sem).wait()

    barrier = pltpu.get_barrier_semaphore()

    def greet(k, carry):
        pl.semaphore_signal(barrier, inc=1, device_id=(plane(k), x), device_id_type=MESH)
        return carry

    loads = [
        pltpu.make_async_copy(src, dst, load_sem.at[n])
        for n, (src, dst) in enumerate(
            [
                (wq_h, wq), (wk_h, wk), (wv_h, wv), (wo_h, wo),
                (dg, gbuf.at[c, x]), (du, ubuf.at[c, x]), (dd, dbuf.at[c, x]),
                (st_h, st), (wm_h, wm), (eg, wg), (eu, wu), (ed, wd),
            ]
        )
    ]
    for load in loads:
        load.start()
    for d in (2, 1, 3):
        pl.semaphore_signal(barrier, inc=1, device_id=(ep, (x + d) % 4), device_id_type=MESH)
    lax.fori_loop(1, 32, greet, 0)

    def first_round(buf, ssem, rsem):
        block = buf.at[c, x]
        copies = [
            remote(block, block, ssem.at[0], rsem.at[0], ep, right),
            remote(block, block, ssem.at[1], rsem.at[1], ep, left),
            remote(block, block, ssem.at[4], rsem.at[4], mate, x),
        ]
        for copy in copies:
            copy.start()
        return copies

    def second_round(buf, ssem, rsem):
        from_left, from_right = buf.at[c, left], buf.at[c, right]
        low = buf.at[c, left, pl.ds(0, 96)]
        high = buf.at[c, right, pl.ds(96, 80)]
        copies = [
            remote(low, low, ssem.at[2], rsem.at[2], ep, right),
            remote(from_left, from_left, ssem.at[5], rsem.at[5], mate, x),
            remote(high, high, ssem.at[3], rsem.at[3], ep, left),
            remote(from_right, from_right, ssem.at[6], rsem.at[6], mate, x),
        ]
        landed(from_left, rsem.at[0])
        copies[0].start()
        copies[1].start()
        landed(from_right, rsem.at[1])
        copies[2].start()
        copies[3].start()
        return copies

    def third_round(buf, ssem, rsem):
        block = buf.at[c, far]
        landed(buf.at[c, far, pl.ds(0, 96)], rsem.at[2])
        landed(buf.at[c, far, pl.ds(96, 80)], rsem.at[3])
        copy = remote(block, block, ssem.at[7], rsem.at[7], mate, x)
        copy.start()
        return [copy]

    def from_mate(buf, rsem):
        for n, place in ((4, x), (5, left), (6, right), (7, far)):
            landed(buf.at[1 - c, place], rsem.at[n])

    start_f = hidden[...].astype(F32)
    start_scale = lax.rsqrt(jnp.sum(start_f * start_f, axis=1, keepdims=True) / 2048.0 + EPS)
    normed_in = (start_f * start_scale * gains[0:1, :]).astype(BF)
    same = iota((32, 32), 0) == iota((32, 32), 1)

    def as_column(row):
        return jnp.sum(jnp.where(same, jnp.broadcast_to(row, (32, 32)), 0.0), axis=1, keepdims=True)

    def as_row(column):
        return jnp.sum(jnp.where(same, jnp.broadcast_to(column, (32, 32)), 0.0), axis=0, keepdims=True)

    def along(a, b):
        return lax.dot_general(a, b, (((1,), (1,)), ((), ())), preferred_element_type=F32)

    gate_in = along(normed_in, w_in[...])
    forget = along(normed_in, w_fg[...]) + bias[...]
    forget = jnp.minimum(forget, 0.0) - jnp.log(1.0 + jnp.exp(-jnp.abs(forget)))
    head8 = iota((32, 8), 1)
    keeps, writes, floors = [], [], []
    for h in range(2):
        mine = head8 == 2 * x + h
        in_gate = jnp.sum(jnp.where(mine, gate_in, 0.0), axis=1, keepdims=True)
        carried = jnp.sum(jnp.where(mine, forget, 0.0), axis=1, keepdims=True) + as_column(smax[h : h + 1, :])
        new_max = jnp.maximum(carried, in_gate)
        keeps.append(jnp.exp(carried - new_max))
        writes.append(jnp.exp(in_gate - new_max))
        floors.append(jnp.exp(-new_max))
        max_out[h : h + 1, :] = as_row(new_max)
    loads[0].wait()
    query = dot(normed_in, wq[...]).astype(BF)
    loads[1].wait()
    keys = dot(normed_in, wk[...]).astype(BF).astype(F32) * 128.0 ** (-0.5)
    loads[2].wait()
    value = dot(normed_in, wv[...]).astype(BF).astype(F32)
    loads[3].wait()
    out_gate = dot(normed_in, wo[...]).astype(BF).astype(F32)

    pl.semaphore_wait(barrier, 34)
    loads[4].wait()
    weight_out = first_round(gbuf, gs_sem, gr_sem)

    eye = same.astype(BF)
    loads[7].wait()
    mixed = []
    for h in range(2):
        lanes = slice(h * 128, (h + 1) * 128)
        query_t = lax.dot_general(
            query[:, lanes], eye, (((0,), (0,)), ((), ())), preferred_element_type=F32
        )
        for s in range(32):
            numer[h, s : s + 1, :] = jnp.sum(
                query_t[:, s : s + 1] * st[s * 2 + h], axis=0, keepdims=True
            )
        q = query[:, lanes].astype(F32)
        written = writes[h] * keys[:, lanes]
        new_norm = keeps[h] * snorm[:, h, :] + written
        top = keeps[h] * numer[h] + jnp.sum(q * written, axis=1, keepdims=True) * value[:, lanes]
        denom = jnp.sum(q * new_norm, axis=1, keepdims=True)
        read = top / jnp.maximum(jnp.abs(denom), floors[h])
        mixed.append((read / (1.0 + jnp.exp(-out_gate[:, lanes]))).astype(BF))
        keep_out[h] = jnp.broadcast_to(keeps[h], (32, 128))
        written_out[h] = written
        value_out[h] = value[:, lanes]
        norm_out[h] = new_norm
    loads[8].wait()
    share = [
        (dot(mixed[0], wm[0:128, q * CH : (q + 1) * CH]) + dot(mixed[1], wm[128:256, q * CH : (q + 1) * CH])).astype(BF)
        for q in range(4)
    ]

    order = one_hot(128, 128, lambda r: ((r >> 3) & 3) * 32 + (r >> 5) * 8 + (r & 7))
    bsend[...] = dot(order, jnp.concatenate(share, axis=0)).astype(BF).reshape(4, 32, CH)
    brecv[x] = bsend[x]
    branch_out = []
    for d in (2, 1, 3):
        to = (x + d) % 4
        branch_out.append(remote(bsend.at[to], brecv.at[x], b_sem.at[0], b_sem.at[1], ep, to))
        branch_out[-1].start()

    loads[5].wait()
    weight_out += first_round(ubuf, us_sem, ur_sem)
    hperm[...] = dot(order, stacked(hidden)).reshape(4, 32, CH)

    expert0, expert1 = as_column(routes[0:1, :].astype(F32)), as_column(routes[1:2, :].astype(F32))
    lane32 = iota((32, 32), 1)
    lane32_f = lane32.astype(F32)
    hot0 = (lane32_f == expert0).astype(F32)
    hot1 = (lane32_f == expert1).astype(F32)
    earlier = (iota((32, 32), 0) > lane32).astype(BF)
    before = dot(earlier, (hot0 + hot1).astype(BF))
    score0, score1 = as_column(scores[0:1, :]), as_column(scores[1:2, :])
    whole = score0 + score1

    def by_piece(column, step):
        return jnp.concatenate(
            [column[xx * 8 : xx * 8 + 8] + q * step for xx in range(4) for q in range(4)], axis=0
        )

    for k, (expert, hot, score) in enumerate(((expert0, hot0, score0), (expert1, hot1, score1))):
        rank = jnp.sum(hot * before, axis=1, keepdims=True)
        place = by_piece((expert * 16.0 + rank).astype(I32), 4)
        gk[k] = (iota((128, 512), 1) == place).astype(BF)
        share_s[k] = jnp.broadcast_to(by_piece(score / whole, 0.0), (128, 128))
    pm[...] = one_hot(512, 512, lambda r: ((r >> 2) & 31) * 16 + (r >> 7) * 4 + (r & 3))
    pmi[...] = one_hot(512, 512, lambda r: ((r >> 2) & 3) * 128 + (r >> 4) * 4 + (r & 3))
    pd[...] = one_hot(512, 512, lambda r: ((r >> 3) & 15) * 32 + (r >> 7) * 8 + (r & 7))
    pdi[...] = one_hot(512, 512, lambda r: ((r >> 3) & 3) * 128 + (r >> 5) * 8 + (r & 7))

    def gain(k):
        return jnp.concatenate(
            [jnp.broadcast_to(gains[k : k + 1, q * CH : (q + 1) * CH], (8, CH)) for q in range(4)],
            axis=0,
        )

    mix_rows = jnp.concatenate(
        [jnp.broadcast_to(mix[0:1, q * CH : (q + 1) * CH], (8, CH)) for q in range(4)], axis=0
    )

    landed(brecv.at[pl.ds(0, 3)], b_sem.at[1])
    branch = brecv[0].astype(F32) + brecv[1].astype(F32) + brecv[2].astype(F32) + brecv[3].astype(F32)
    branch = branch.astype(BF).astype(F32)
    residual_f = hperm[x] + gain(1) * branch * lax.rsqrt(row_total(branch * branch) / 2048.0 + EPS)
    scale_two = lax.rsqrt(row_total(residual_f * residual_f) / 2048.0 + EPS)
    normed = (residual_f * scale_two * gain(2)).astype(BF)
    nall[x] = normed
    tok[p] = normed

    token_out = []
    for d in (2, 1, 3):
        to = (x + d) % 4
        token_out.append(remote(nall.at[x], nall.at[x], n_sem.at[0], n_sem.at[1], ep, to))
        token_out[-1].start()

    def share_tokens(k, carry):
        to = ((z + k // 4) % 4) * 8 + ((y + k % 4) % 4) * 2 + c
        remote(nall.at[x], tok.at[p], t_sem.at[0], t_sem.at[1], to, x).start()
        return carry

    lax.fori_loop(1, 16, share_tokens, 0)
    weight_out += second_round(gbuf, gs_sem, gr_sem)
    resid_s[...] = residual_f.astype(BF).astype(F32)
    mix_dot = scale_two * row_total(residual_f * gain(2) * mix_rows)
    mixg_s[...] = jnp.broadcast_to(1.0 / (1.0 + jnp.exp(-mix_dot)), (32, 128))

    landed(nall.at[pl.ds(0, 3)], n_sem.at[1])
    chosen = gk[0] + gk[1]
    rows = lax.dot_general(
        chosen, nall[...].reshape(128, CH), (((0,), (0,)), ((), ())), preferred_element_type=F32
    )
    osend[...] = rows.astype(BF).reshape(32, 16, CH)
    orecv[ep] = osend[ep]

    def dispatch(k, carry):
        to = plane(k)
        remote(osend.at[to], orecv.at[ep], o_sem.at[0], o_sem.at[1], to, x).start()
        return carry

    lax.fori_loop(1, 32, dispatch, 0)

    loads[6].wait()
    weight_out += second_round(ubuf, us_sem, ur_sem)
    weight_out += first_round(dbuf, ds_sem, dr_sem)
    weight_out += third_round(gbuf, gs_sem, gr_sem)
    weight_out += third_round(ubuf, us_sem, ur_sem)
    weight_out += second_round(dbuf, ds_sem, dr_sem)

    landed(tok.at[pl.ds(0, 15)], t_sem.at[1])
    xd[...] = dot(pd[...], tok[...].reshape(512, CH)).astype(BF).reshape(4, 128, CH)
    from_mate(gbuf, gr_sem)
    from_mate(ubuf, ur_sem)
    for core in range(2):
        pre_gate = along(xd[0], gbuf[core, 0])
        pre_up = along(xd[0], ubuf[core, 0])
        for q in range(1, 4):
            pre_gate += along(xd[q], gbuf[core, q])
            pre_up += along(xd[q], ubuf[core, q])
        hden[core] = (silu(pre_gate) * pre_up).astype(BF)
    weight_out += third_round(dbuf, ds_sem, dr_sem)
    from_mate(dbuf, dr_sem)
    for q in range(4):
        yd[q * 128 : (q + 1) * 128] = (
            dot(hden[0], dbuf[0, q]) + dot(hden[1], dbuf[1, q])
        ).astype(BF)
    dsend[...] = dot(pdi[...], yd[...]).astype(BF).reshape(16, 32, CH)
    drecv[p] = dsend[p]

    def dense_back(k, carry):
        to = ((z + k // 4) % 4) * 4 + (y + k % 4) % 4
        remote(dsend.at[to], drecv.at[p], d_sem.at[0], d_sem.at[1], to * 2 + c, x).start()
        return carry

    lax.fori_loop(1, 16, dense_back, 0)

    landed(orecv.at[pl.ds(0, 31)], o_sem.at[1])
    xs[...] = dot(pm[...], orecv[...].reshape(512, CH)).astype(BF).reshape(4, 128, CH)
    loads[9].wait()
    loads[10].wait()
    gate_pre = dot(xs[0], wg[0])
    up_pre = dot(xs[0], wu[0])
    for q in range(1, 4):
        gate_pre += dot(xs[q], wg[q])
        up_pre += dot(xs[q], wu[q])
    hexp[...] = (silu(gate_pre) * up_pre).astype(BF)
    loads[11].wait()
    for q in range(4):
        ys[q * 128 : (q + 1) * 128] = dot(hexp[...], wd[:, q * CH : (q + 1) * CH]).astype(BF)
    rsend[...] = dot(pmi[...], ys[...]).astype(BF).reshape(32, 16, CH)
    rrecv[ep] = rsend[ep]

    def give_back(k, carry):
        to = plane(k)
        remote(rsend.at[to], rrecv.at[ep], r_sem.at[0], r_sem.at[1], to, x).start()
        return carry

    lax.fori_loop(1, 32, give_back, 0)

    landed(rrecv.at[pl.ds(0, 31)], r_sem.at[1])
    back = rrecv[...].reshape(512, CH)
    moe = share_s[0][:, 0:1] * dot(gk[0], back) + share_s[1][:, 0:1] * dot(gk[1], back)
    msend[...] = moe.astype(BF).reshape(4, 32, CH)
    mrecv[x] = msend[x]
    moe_out = []
    for d in (2, 1, 3):
        to = (x + d) % 4
        moe_out.append(remote(msend.at[to], mrecv.at[x], m_sem.at[0], m_sem.at[1], ep, to))
        moe_out[-1].start()

    landed(drecv.at[pl.ds(0, 15)], d_sem.at[1])
    dense = drecv[0].astype(F32)
    for n in range(1, 16):
        dense += drecv[n].astype(F32)
    landed(mrecv.at[pl.ds(0, 3)], m_sem.at[1])
    ffn = mrecv[0].astype(F32) + mrecv[1].astype(F32) + mrecv[2].astype(F32) + mrecv[3].astype(F32)
    ffn += mixg_s[:, 0:1] * dense
    scale_ffn = lax.rsqrt(row_total(ffn * ffn) / 2048.0 + EPS)
    fsend[...] = (resid_s[...] + gain(3) * ffn * scale_ffn).reshape(4, 8, CH)
    frecv[x] = fsend[x]
    last_out = []
    for d in (2, 1, 3):
        to = (x + d) % 4
        last_out.append(remote(fsend.at[to], frecv.at[x], f_sem.at[0], f_sem.at[1], ep, to))
        last_out[-1].start()

    for copy in weight_out:
        copy.wait_send()
    landed(bsend.at[pl.ds(0, 3)], b_sem.at[0])
    landed(nall.at[pl.ds(0, 3)], n_sem.at[0])
    landed(tok.at[pl.ds(0, 15)], t_sem.at[0])
    landed(osend.at[pl.ds(0, 31)], o_sem.at[0])
    landed(rsend.at[pl.ds(0, 31)], r_sem.at[0])
    landed(dsend.at[pl.ds(0, 15)], d_sem.at[0])
    landed(msend.at[pl.ds(0, 3)], m_sem.at[0])
    landed(frecv.at[pl.ds(0, 3)], f_sem.at[1])
    out[...] = frecv[...].reshape(32, CH).astype(BF)
    landed(fsend.at[pl.ds(0, 3)], f_sem.at[0])


def whole(small, large):
    V = pltpu.VMEM
    dma = pltpu.SemaphoreType.DMA
    vm = pl.BlockSpec(memory_space=pltpu.VMEM)
    hb = pl.BlockSpec(memory_space=pl.ANY)
    head = jax.ShapeDtypeStruct((2, 32, 128), F32)
    return pl.pallas_call(
        whole_kernel,
        out_shape=(
            jax.ShapeDtypeStruct((32, CH), BF), head, head, head, head,
            jax.ShapeDtypeStruct((2, 32), F32),
        ),
        in_specs=[vm] * len(small) + [hb] * len(large),
        out_specs=(vm,) * 6,
        scratch_shapes=[
            V((2048, 256), BF), V((2048, 256), BF), V((2048, 256), BF), V((2048, 256), BF),
            V((256, 2048), BF), V((64, 128, 128), F32), V((2, 32, 128), F32),
            V((4, 512, 896), BF), V((4, 512, 896), BF), V((896, 2048), BF),
            V((2, 4, 176, 512), BF), V((2, 4, 176, 512), BF), V((2, 4, 176, 512), BF),
            V((4, 32, CH), BF), V((4, 32, CH), BF), V((4, 32, CH), F32), V((4, 32, CH), BF),
            V((16, 32, CH), BF),
            V((32, 16, CH), BF), V((32, 16, CH), BF), V((32, 16, CH), BF), V((32, 16, CH), BF),
            V((16, 32, CH), BF), V((16, 32, CH), BF),
            V((4, 32, CH), BF), V((4, 32, CH), BF), V((4, 8, CH), F32), V((4, 8, CH), F32),
            V((512, 512), BF), V((512, 512), BF), V((512, 512), BF), V((512, 512), BF),
            V((2, 128, 512), BF), V((4, 128, CH), BF), V((4, 128, CH), BF),
            V((512, CH), BF), V((512, CH), BF), V((128, 896), BF), V((2, 128, 176), BF),
            V((32, CH), F32), V((32, 128), F32), V((2, 128, 128), F32),
            dma((12,)), dma((2,)), dma((2,)), dma((2,)), dma((2,)), dma((2,)), dma((2,)),
            dma((2,)), dma((2,)), dma((8,)), dma((8,)), dma((8,)), dma((8,)), dma((8,)), dma((8,)),
        ],
        compiler_params=pltpu.CompilerParams(
            collective_id=0, has_side_effects=True, vmem_limit_bytes=60 * 1024 * 1024
        ),
        name="whole",
    )(*small, *large)


def memory_kernel(
    state, keep, written, value, norm, top, hidden_in, matrix_out, norm_out, top_out, hidden_out
):
    spot = iota((8, 128), 0)
    for h in range(2):
        w = written[h]
        high = w.astype(BF).astype(F32)
        low = w - high
        both = jnp.concatenate([value[h], value[h]], axis=0).astype(BF)
        norm_out[:, h, :] = norm[h]
        for s in range(8):
            sides = jnp.concatenate(
                [jnp.where(spot == s, high, 0.0), jnp.where(spot == s, low, 0.0)], axis=0
            ).astype(BF)
            outer = lax.dot_general(sides, both, (((0,), (0,)), ((), ())), preferred_element_type=F32)
            matrix_out[s, h] = keep[h, s : s + 1, :] * state[s, h] + outer
    top_out[...] = top[...]
    hidden_out[...] = hidden_in[...]


def memory(state, keep, written, value, norm, top, hidden_in):
    part = pl.BlockSpec((2, 8, 128), lambda n: (0, n, 0))
    fixed2 = pl.BlockSpec((2, 32), lambda n: (0, 0))
    fixed = pl.BlockSpec((32, CH), lambda n: (0, 0))
    block = pl.BlockSpec((8, 2, 128, 128), lambda n: (n, 0, 0, 0))
    return pl.pallas_call(
        memory_kernel,
        grid=(4,),
        out_shape=(
            jax.ShapeDtypeStruct((32, 2, 128, 128), F32),
            jax.ShapeDtypeStruct((32, 2, 128), F32),
            jax.ShapeDtypeStruct((2, 32), F32),
            jax.ShapeDtypeStruct((32, CH), BF),
        ),
        in_specs=[block, part, part, part, part, fixed2, fixed],
        out_specs=(block, pl.BlockSpec((8, 2, 128), lambda n: (n, 0, 0)), fixed2, fixed),
        name="memory",
    )(state, keep, written, value, norm, top, hidden_in)


def local(
    hidden,
    norm_gains,
    w_query,
    w_key,
    w_value,
    w_outgate,
    w_input_gate,
    w_forget_gate,
    forget_bias,
    w_mix_out,
    state_matrix,
    state_norm,
    state_max,
    routes,
    route_scores,
    expert_gate,
    expert_up,
    expert_down,
    dense_gate,
    dense_up,
    dense_down,
    dense_mix,
):
    new_hidden, keep, written, value, norm, top = whole(
        (
            hidden, norm_gains, dense_mix.reshape(1, -1), routes.T, route_scores.T,
            w_input_gate.T, w_forget_gate.T, forget_bias.reshape(1, -1), state_max.T, state_norm,
        ),
        (
            w_query, w_key, w_value, w_outgate, w_mix_out, state_matrix.reshape(64, 128, 128),
            expert_gate.reshape(4, CH, -1), expert_up.reshape(4, CH, -1), expert_down[0],
            dense_gate.T, dense_up.T, dense_down,
        ),
    )
    new_matrix, new_norm, new_top, new_hidden = memory(
        state_matrix, keep, written, value, norm, top, new_hidden
    )
    return (new_hidden, new_matrix, new_norm, new_top.T)


def solution(mesh):
    placed = (
        P("ep", None),
        P(),
        P(None, "tp"),
        P(None, "tp"),
        P(None, "tp"),
        P(None, "tp"),
        P(),
        P(),
        P(),
        P("tp", None),
        P("ep", "tp", None, None),
        P("ep", "tp", None),
        P("ep", "tp"),
        P("ep", None),
        P("ep", None),
        P("ep", None, "tp"),
        P("ep", None, "tp"),
        P("ep", "tp", None),
        P("tp", "ep"),
        P("tp", "ep"),
        P("ep", "tp"),
        P(),
    )
    return jax.shard_map(
        local,
        mesh=mesh,
        in_specs=placed,
        out_specs=(P("ep", "tp"), P("ep", "tp", None, None), P("ep", "tp", None), P("ep", "tp")),
        check_vma=False,
    )
```

```python
import jax
import jax.numpy as jnp
from jax import lax
from jax.experimental import pallas as pl
from jax.experimental.pallas import tpu as pltpu
from jax.sharding import PartitionSpec as P

EPS = 1e-06
MESH = pl.DeviceIdType.MESH
BF = jnp.bfloat16
F32 = jnp.float32
I32 = jnp.int32
CHIP_STEPS = sorted(
    ((dz, dy) for dz in range(4) for dy in range(4) if dz or dy),
    key=lambda s: -(min(s[0], 4 - s[0]) + min(s[1], 4 - s[1])),
)
PIECES = ((0, 96), (96, 80))
CH = 512


def dot(a, b):
    return jnp.dot(a, b, preferred_element_type=F32)


def iota(shape, dim):
    return lax.broadcasted_iota(I32, shape, dim)


def one_hot(columns, rows, target):
    return (iota((rows, columns), 1) == target(iota((rows, columns), 0))).astype(BF)


def stacked(ref):
    return jnp.concatenate([ref[:, q * CH : (q + 1) * CH] for q in range(4)], axis=0)


def row_total(values):
    part = jnp.sum(values, axis=1, keepdims=True)
    total = part[0:8] + part[8:16] + part[16:24] + part[24:32]
    return jnp.concatenate([total] * 4, axis=0)


def silu(t):
    return t / (1.0 + jnp.exp(-t))


def whole_kernel(
    hidden_h, gains_h, mix_h, routes_h, scores_h, w_in_h, w_fg_h, bias_h, smax_h, snorm_h,
    wq_h, wk_h, wv_h, wo_h, wm_h, st_h, eg, eu, ed, dg, du, dd,
    out, matrix, norm_out, max_out,
    hidden, gains, mix, routes, scores, w_in, w_fg, bias, smax, snorm,
    wq, wk, wv, wo, wm, st, numer,
    wg, wu, wd, gbuf, ubuf, dbuf,
    bsend, brecv, hperm, nall, tok, osend, orecv, rsend, rrecv, dsend, drecv,
    msend, mrecv, fsend, frecv,
    pm, pmi, pd, pdi, gk, xs, xd, ys, yd, hexp, hden, resid_s, mixg_s, share_s,
    load_sem, b_sem, n_sem, t_sem, o_sem, r_sem, d_sem, m_sem, f_sem,
    gs_sem, gr_sem, us_sem, ur_sem, ds_sem, dr_sem,
):
    x = lax.axis_index("tp")
    ep = lax.axis_index("ep")
    c = ep % 2
    y = (ep // 2) % 4
    z = ep // 8
    p = ep // 2
    mate = p * 2 + (1 - c)
    left, right, far = (x + 3) % 4, (x + 1) % 4, (x + 2) % 4

    z_at = [((z + d) % 4) * 8 for d in range(4)]
    y_at = [((y + d) % 4) * 2 for d in range(4)]
    core_at = [c, 1 - c]
    places = [((z + dz) % 4) * 4 + (y + dy) % 4 for dz, dy in CHIP_STEPS]
    chips = [z_at[dz] + y_at[dy] for dz, dy in CHIP_STEPS]
    peers = [base + core for base in chips for core in core_at]
    peers.append(p * 2 + core_at[1])

    def remote(src, dst, ssem, rsem, to_ep, to_x):
        return pltpu.make_async_remote_copy(
            src_ref=src, dst_ref=dst, send_sem=ssem, recv_sem=rsem,
            device_id=(to_ep, to_x), device_id_type=MESH,
        )

    def landed(ref, sem):
        pltpu.make_async_copy(ref, ref, sem).wait()

    barrier = pltpu.get_barrier_semaphore()

    loads = {
        name: pltpu.make_async_copy(src, dst, load_sem.at[n])
        for n, (name, src, dst) in enumerate(
            [
                ("hidden", hidden_h, hidden), ("gains", gains_h, gains),
                ("wq", wq_h, wq), ("wk", wk_h, wk), ("w_in", w_in_h, w_in), ("w_fg", w_fg_h, w_fg),
                ("bias", bias_h, bias), ("smax", smax_h, smax), ("wv", wv_h, wv), ("wo", wo_h, wo),
                ("gate", dg, gbuf.at[c, x]), ("st", st_h, st), ("snorm", snorm_h, snorm), ("wm", wm_h, wm),
                ("up", du, ubuf.at[c, x]), ("down", dd, dbuf.at[c, x]), ("mix", mix_h, mix),
                ("routes", routes_h, routes), ("scores", scores_h, scores),
                ("eg", eg, wg), ("eu", eu, wu), ("ed", ed, wd),
            ]
        )
    }
    for name in ("hidden", "gains", "wq", "wk"):
        loads[name].start()
    for d in (2, 1, 3):
        pl.semaphore_signal(barrier, inc=1, device_id=(ep, (x + d) % 4), device_id_type=MESH)
    for peer in peers:
        pl.semaphore_signal(barrier, inc=1, device_id=(peer, x), device_id_type=MESH)
    for name, load in loads.items():
        if name not in ("hidden", "gains", "wq", "wk"):
            load.start()

    def first_round(weight, part):
        buf, ssem, rsem = weight
        copies = []
        for piece, to in ((0, right), (1, left)) if part == 0 else ((1, right), (0, left)):
            block = buf.at[c, x, pl.ds(*PIECES[piece])]
            n = 2 * part + piece
            copies.append(remote(block, block, ssem.at[n], rsem.at[n], ep, to))
        if part == 1:
            block = buf.at[c, x]
            copies.append(remote(block, block, ssem.at[6], rsem.at[6], mate, x))
        for copy in copies:
            copy.start()
        return copies

    def second_round(weight):
        buf, ssem, rsem = weight
        copies = []
        for piece, near, onward in ((0, left, right), (1, right, left)):
            block = buf.at[c, near, pl.ds(*PIECES[piece])]
            landed(block, rsem.at[piece])
            copies.append(remote(block, block, ssem.at[4 + piece], rsem.at[4 + piece], ep, onward))
            copies[-1].start()
        return copies

    def near_to_mate(weight):
        buf, ssem, rsem = weight
        copies = []
        for piece, n, near in ((1, 7, left), (0, 8, right)):
            landed(buf.at[c, near, pl.ds(*PIECES[piece])], rsem.at[2 + piece])
            block = buf.at[c, near]
            copies.append(remote(block, block, ssem.at[n], rsem.at[n], mate, x))
            copies[-1].start()
        return copies

    def far_to_mate(weight):
        buf, ssem, rsem = weight
        copies = []
        for piece in range(2):
            block = buf.at[c, far, pl.ds(*PIECES[piece])]
            landed(block, rsem.at[4 + piece])
            copies.append(remote(block, block, ssem.at[9 + piece], rsem.at[9 + piece], mate, x))
            copies[-1].start()
        return copies

    def from_mate(weight):
        buf, _, rsem = weight
        for n, place in ((6, x), (7, left), (8, right)):
            landed(buf.at[1 - c, place], rsem.at[n])
        for piece in range(2):
            landed(buf.at[1 - c, far, pl.ds(*PIECES[piece])], rsem.at[9 + piece])

    gate_w = (gbuf, gs_sem, gr_sem)
    up_w = (ubuf, us_sem, ur_sem)
    down_w = (dbuf, ds_sem, dr_sem)

    loads["hidden"].wait()
    start_f = hidden[...].astype(F32)
    start_scale = lax.rsqrt(jnp.sum(start_f * start_f, axis=1, keepdims=True) / 2048.0 + EPS)
    loads["gains"].wait()
    normed_in = (start_f * start_scale * gains[0:1, :]).astype(BF)
    same = iota((32, 32), 0) == iota((32, 32), 1)

    def as_column(row):
        return jnp.sum(jnp.where(same, jnp.broadcast_to(row, (32, 32)), 0.0), axis=1, keepdims=True)

    def as_row(column):
        return jnp.sum(jnp.where(same, jnp.broadcast_to(column, (32, 32)), 0.0), axis=0, keepdims=True)

    def along(a, b):
        return lax.dot_general(a, b, (((1,), (1,)), ((), ())), preferred_element_type=F32)

    loads["wq"].wait()
    query = dot(normed_in, wq[...]).astype(BF)
    loads["wk"].wait()
    keys = dot(normed_in, wk[...]).astype(BF).astype(F32) * 128.0 ** (-0.5)
    for name in ("w_in", "w_fg", "bias", "smax"):
        loads[name].wait()
    gate_in = along(normed_in, w_in[...])
    forget = along(normed_in, w_fg[...]) + bias[...]
    forget = jnp.minimum(forget, 0.0) - jnp.log(1.0 + jnp.exp(-jnp.abs(forget)))
    head8 = iota((32, 8), 1)
    keeps, writes, floors = [], [], []
    for h in range(2):
        mine = head8 == 2 * x + h
        in_gate = jnp.sum(jnp.where(mine, gate_in, 0.0), axis=1, keepdims=True)
        carried = jnp.sum(jnp.where(mine, forget, 0.0), axis=1, keepdims=True) + as_column(smax[h : h + 1, :])
        new_max = jnp.maximum(carried, in_gate)
        keeps.append(jnp.exp(carried - new_max))
        writes.append(jnp.exp(in_gate - new_max))
        floors.append(jnp.exp(-new_max))
        max_out[h : h + 1, :] = as_row(new_max)
    loads["wv"].wait()
    value = dot(normed_in, wv[...]).astype(BF).astype(F32)
    loads["wo"].wait()
    out_gate = dot(normed_in, wo[...]).astype(BF).astype(F32)

    pl.semaphore_wait(barrier, 34)
    loads["gate"].wait()
    weight_out = first_round(gate_w, 0)

    eye = same.astype(BF)
    loads["st"].wait()
    loads["snorm"].wait()
    mixed, written_t = [], []
    for h in range(2):
        lanes = slice(h * 128, (h + 1) * 128)
        query_t = lax.dot_general(
            query[:, lanes], eye, (((0,), (0,)), ((), ())), preferred_element_type=F32
        )
        for s in range(32):
            numer[h, s : s + 1, :] = jnp.sum(
                query_t[:, s : s + 1] * st[s * 2 + h], axis=0, keepdims=True
            )
        q = query[:, lanes].astype(F32)
        written = writes[h] * keys[:, lanes]
        new_norm = keeps[h] * snorm[:, h, :] + written
        top = keeps[h] * numer[h] + jnp.sum(q * written, axis=1, keepdims=True) * value[:, lanes]
        denom = jnp.sum(q * new_norm, axis=1, keepdims=True)
        read = top / jnp.maximum(jnp.abs(denom), floors[h])
        mixed.append((read / (1.0 + jnp.exp(-out_gate[:, lanes]))).astype(BF))
        written_t.append(jnp.transpose(written))
        norm_out[h] = new_norm
    loads["wm"].wait()
    share = [
        (dot(mixed[0], wm[0:128, q * CH : (q + 1) * CH]) + dot(mixed[1], wm[128:256, q * CH : (q + 1) * CH])).astype(BF)
        for q in range(4)
    ]

    order = one_hot(128, 128, lambda r: ((r >> 3) & 3) * 32 + (r >> 5) * 8 + (r & 7))
    bsend[...] = dot(order, jnp.concatenate(share, axis=0)).astype(BF).reshape(4, 32, CH)
    brecv[x] = bsend[x]
    branch_out = []
    for d in (2, 1, 3):
        to = (x + d) % 4
        branch_out.append(remote(bsend.at[to], brecv.at[x], b_sem.at[0], b_sem.at[1], ep, to))
        branch_out[-1].start()

    weight_out += first_round(gate_w, 1)
    hperm[...] = dot(order, stacked(hidden)).reshape(4, 32, CH)

    for name in ("mix", "routes", "scores"):
        loads[name].wait()
    expert0, expert1 = as_column(routes[0:1, :].astype(F32)), as_column(routes[1:2, :].astype(F32))
    lane32 = iota((32, 32), 1)
    lane32_f = lane32.astype(F32)
    hot0 = (lane32_f == expert0).astype(F32)
    hot1 = (lane32_f == expert1).astype(F32)
    earlier = (iota((32, 32), 0) > lane32).astype(BF)
    before = dot(earlier, (hot0 + hot1).astype(BF))
    score0, score1 = as_column(scores[0:1, :]), as_column(scores[1:2, :])
    whole = score0 + score1

    def by_piece(column, step):
        return jnp.concatenate(
            [column[xx * 8 : xx * 8 + 8] + q * step for xx in range(4) for q in range(4)], axis=0
        )

    for k, (expert, hot, score) in enumerate(((expert0, hot0, score0), (expert1, hot1, score1))):
        rank = jnp.sum(hot * before, axis=1, keepdims=True)
        place = by_piece((expert * 16.0 + rank).astype(I32), 4)
        gk[k] = (iota((128, 512), 1) == place).astype(BF)
        share_s[k] = jnp.broadcast_to(by_piece(score / whole, 0.0), (128, 128))
    pm[...] = one_hot(512, 512, lambda r: ((r >> 2) & 31) * 16 + (r >> 7) * 4 + (r & 3))
    pmi[...] = one_hot(512, 512, lambda r: ((r >> 2) & 3) * 128 + (r >> 4) * 4 + (r & 3))
    pd[...] = one_hot(512, 512, lambda r: ((r >> 3) & 15) * 32 + (r >> 7) * 8 + (r & 7))
    pdi[...] = one_hot(512, 512, lambda r: ((r >> 3) & 3) * 128 + (r >> 5) * 8 + (r & 7))

    def gain(k):
        return jnp.concatenate(
            [jnp.broadcast_to(gains[k : k + 1, q * CH : (q + 1) * CH], (8, CH)) for q in range(4)],
            axis=0,
        )

    mix_rows = jnp.concatenate(
        [jnp.broadcast_to(mix[0:1, q * CH : (q + 1) * CH], (8, CH)) for q in range(4)], axis=0
    )

    for h in range(2):
        for s in range(32):
            matrix[s, h] = (
                keeps[h][s : s + 1, :] * st[s * 2 + h]
                + written_t[h][:, s : s + 1] * value[s : s + 1, h * 128 : (h + 1) * 128]
            )

    landed(brecv.at[pl.ds(0, 3)], b_sem.at[1])
    branch = brecv[0].astype(F32) + brecv[1].astype(F32) + brecv[2].astype(F32) + brecv[3].astype(F32)
    branch = branch.astype(BF).astype(F32)
    residual_f = hperm[x] + gain(1) * branch * lax.rsqrt(row_total(branch * branch) / 2048.0 + EPS)
    scale_two = lax.rsqrt(row_total(residual_f * residual_f) / 2048.0 + EPS)
    normed = (residual_f * scale_two * gain(2)).astype(BF)
    nall[x] = normed
    tok[p] = normed

    token_out = []
    for d in (2, 1, 3):
        to = (x + d) % 4
        token_out.append(remote(nall.at[x], nall.at[x], n_sem.at[0], n_sem.at[1], ep, to))
        token_out[-1].start()

    for chip in chips:
        remote(nall.at[x], tok.at[p], t_sem.at[0], t_sem.at[1], chip + c, x).start()
    loads["up"].wait()
    loads["down"].wait()
    weight_out += first_round(up_w, 0) + first_round(up_w, 1)
    weight_out += second_round(gate_w)
    resid_s[...] = residual_f.astype(BF).astype(F32)
    mix_dot = scale_two * row_total(residual_f * gain(2) * mix_rows)
    mixg_s[...] = jnp.broadcast_to(1.0 / (1.0 + jnp.exp(-mix_dot)), (32, 128))

    landed(nall.at[pl.ds(0, 3)], n_sem.at[1])
    chosen = gk[0] + gk[1]
    rows = lax.dot_general(
        chosen, nall[...].reshape(128, CH), (((0,), (0,)), ((), ())), preferred_element_type=F32
    )
    osend[...] = rows.astype(BF).reshape(32, 16, CH)
    orecv[ep] = osend[ep]

    for peer in peers:
        remote(osend.at[peer], orecv.at[ep], o_sem.at[0], o_sem.at[1], peer, x).start()
    weight_out += near_to_mate(gate_w)
    weight_out += second_round(up_w)
    weight_out += first_round(down_w, 0) + first_round(down_w, 1)
    weight_out += near_to_mate(up_w)
    weight_out += far_to_mate(gate_w)
    weight_out += far_to_mate(up_w)

    landed(tok.at[pl.ds(0, 15)], t_sem.at[1])
    xd[...] = dot(pd[...], tok[...].reshape(512, CH)).astype(BF).reshape(4, 128, CH)
    from_mate(gate_w)
    from_mate(up_w)
    for core in range(2):
        pre_gate = along(xd[0], gbuf[core, 0])
        pre_up = along(xd[0], ubuf[core, 0])
        for q in range(1, 4):
            pre_gate += along(xd[q], gbuf[core, q])
            pre_up += along(xd[q], ubuf[core, q])
        hden[core] = (silu(pre_gate) * pre_up).astype(BF)
    weight_out += second_round(down_w)
    weight_out += near_to_mate(down_w)

    landed(orecv.at[pl.ds(0, 31)], o_sem.at[1])
    xs[...] = dot(pm[...], orecv[...].reshape(512, CH)).astype(BF).reshape(4, 128, CH)
    loads["eg"].wait()
    loads["eu"].wait()
    gate_pre = dot(xs[0], wg[0])
    up_pre = dot(xs[0], wu[0])
    for q in range(1, 4):
        gate_pre += dot(xs[q], wg[q])
        up_pre += dot(xs[q], wu[q])
    hexp[...] = (silu(gate_pre) * up_pre).astype(BF)
    loads["ed"].wait()
    for q in range(4):
        ys[q * 128 : (q + 1) * 128] = dot(hexp[...], wd[:, q * CH : (q + 1) * CH]).astype(BF)
    rsend[...] = dot(pmi[...], ys[...]).astype(BF).reshape(32, 16, CH)
    rrecv[ep] = rsend[ep]

    for peer in peers:
        remote(rsend.at[peer], rrecv.at[ep], r_sem.at[0], r_sem.at[1], peer, x).start()

    weight_out += far_to_mate(down_w)
    from_mate(down_w)
    for q in range(4):
        yd[q * 128 : (q + 1) * 128] = (
            dot(hden[0], dbuf[0, q]) + dot(hden[1], dbuf[1, q])
        ).astype(BF)
    dsend[...] = dot(pdi[...], yd[...]).astype(BF).reshape(16, 32, CH)
    drecv[p] = dsend[p]

    for chip, place in zip(chips, places):
        remote(dsend.at[place], drecv.at[p], d_sem.at[0], d_sem.at[1], chip + c, x).start()

    landed(rrecv.at[pl.ds(0, 31)], r_sem.at[1])
    back = rrecv[...].reshape(512, CH)
    moe = share_s[0][:, 0:1] * dot(gk[0], back) + share_s[1][:, 0:1] * dot(gk[1], back)
    msend[...] = moe.astype(BF).reshape(4, 32, CH)
    mrecv[x] = msend[x]
    moe_out = []
    for d in (2, 1, 3):
        to = (x + d) % 4
        moe_out.append(remote(msend.at[to], mrecv.at[x], m_sem.at[0], m_sem.at[1], ep, to))
        moe_out[-1].start()

    landed(drecv.at[pl.ds(0, 15)], d_sem.at[1])
    dense = drecv[0].astype(F32)
    for n in range(1, 16):
        dense += drecv[n].astype(F32)
    landed(mrecv.at[pl.ds(0, 3)], m_sem.at[1])
    ffn = mrecv[0].astype(F32) + mrecv[1].astype(F32) + mrecv[2].astype(F32) + mrecv[3].astype(F32)
    ffn += mixg_s[:, 0:1] * dense
    scale_ffn = lax.rsqrt(row_total(ffn * ffn) / 2048.0 + EPS)
    fsend[...] = (resid_s[...] + gain(3) * ffn * scale_ffn).reshape(4, 8, CH)
    frecv[x] = fsend[x]
    last_out = []
    for d in (2, 1, 3):
        to = (x + d) % 4
        last_out.append(remote(fsend.at[to], frecv.at[x], f_sem.at[0], f_sem.at[1], ep, to))
        last_out[-1].start()

    for copy in weight_out:
        copy.wait_send()
    landed(bsend.at[pl.ds(0, 3)], b_sem.at[0])
    landed(nall.at[pl.ds(0, 3)], n_sem.at[0])
    landed(tok.at[pl.ds(0, 15)], t_sem.at[0])
    landed(osend.at[pl.ds(0, 31)], o_sem.at[0])
    landed(rsend.at[pl.ds(0, 31)], r_sem.at[0])
    landed(dsend.at[pl.ds(0, 15)], d_sem.at[0])
    landed(msend.at[pl.ds(0, 3)], m_sem.at[0])
    landed(frecv.at[pl.ds(0, 3)], f_sem.at[1])
    out[...] = frecv[...].reshape(32, CH).astype(BF)
    landed(fsend.at[pl.ds(0, 3)], f_sem.at[0])


def whole(*arrays):
    V = pltpu.VMEM
    dma = pltpu.SemaphoreType.DMA
    vm = pl.BlockSpec(memory_space=pltpu.VMEM)
    hb = pl.BlockSpec(memory_space=pltpu.HBM)
    return pl.pallas_call(
        whole_kernel,
        out_shape=(
            V((32, CH), BF), V((32, 2, 128, 128), F32), V((2, 32, 128), F32), V((2, 32), F32),
        ),
        in_specs=[hb] * len(arrays),
        out_specs=(vm,) * 4,
        scratch_shapes=[
            V((32, 2048), BF), V((4, 2048), F32), V((1, 2048), F32), V((2, 32), I32), V((2, 32), F32),
            V((8, 2048), BF), V((8, 2048), BF), V((1, 8), F32), V((2, 32), F32), V((32, 2, 128), F32),
            V((2048, 256), BF), V((2048, 256), BF), V((2048, 256), BF), V((2048, 256), BF),
            V((256, 2048), BF), V((64, 128, 128), F32), V((2, 32, 128), F32),
            V((4, 512, 896), BF), V((4, 512, 896), BF), V((896, 2048), BF),
            V((2, 4, 176, 512), BF), V((2, 4, 176, 512), BF), V((2, 4, 176, 512), BF),
            V((4, 32, CH), BF), V((4, 32, CH), BF), V((4, 32, CH), F32), V((4, 32, CH), BF),
            V((16, 32, CH), BF),
            V((32, 16, CH), BF), V((32, 16, CH), BF), V((32, 16, CH), BF), V((32, 16, CH), BF),
            V((16, 32, CH), BF), V((16, 32, CH), BF),
            V((4, 32, CH), BF), V((4, 32, CH), BF), V((4, 8, CH), F32), V((4, 8, CH), F32),
            V((512, 512), BF), V((512, 512), BF), V((512, 512), BF), V((512, 512), BF),
            V((2, 128, 512), BF), V((4, 128, CH), BF), V((4, 128, CH), BF),
            V((512, CH), BF), V((512, CH), BF), V((128, 896), BF), V((2, 128, 176), BF),
            V((32, CH), F32), V((32, 128), F32), V((2, 128, 128), F32),
            dma((22,)), dma((2,)), dma((2,)), dma((2,)), dma((2,)), dma((2,)), dma((2,)),
            dma((2,)), dma((2,)),
            dma((11,)), dma((11,)), dma((11,)), dma((11,)), dma((11,)), dma((11,)),
        ],
        compiler_params=pltpu.CompilerParams(
            collective_id=0, has_side_effects=True, vmem_limit_bytes=44 * 1024 * 1024
        ),
        name="whole",
    )(*(pltpu.with_memory_space_constraint(a, pltpu.HBM) for a in arrays))


def memory_kernel(matrix, norm, top, hidden_in, norm_out, top_out, hidden_out, matrix_h, out_sem):
    stores = [
        pltpu.make_async_copy(matrix.at[pl.ds(n * 4, 4)], matrix_h.at[pl.ds(n * 4, 4)], out_sem.at[n])
        for n in range(8)
    ]
    for store in stores:
        store.start()
    for h in range(2):
        norm_out[:, h, :] = norm[h]
    top_out[...] = top[...]
    hidden_out[...] = hidden_in[...]
    for store in stores:
        store.wait()


def memory(matrix, norm, top, hidden_in):
    vm = pl.BlockSpec(memory_space=pltpu.VMEM)
    return pl.pallas_call(
        memory_kernel,
        out_shape=(
            jax.ShapeDtypeStruct((32, 2, 128), F32),
            jax.ShapeDtypeStruct((2, 32), F32),
            jax.ShapeDtypeStruct((32, CH), BF),
            pltpu.HBM((32, 2, 128, 128), F32),
        ),
        in_specs=[vm] * 4,
        out_specs=(vm, vm, vm, pl.BlockSpec(memory_space=pltpu.HBM)),
        scratch_shapes=[pltpu.SemaphoreType.DMA((8,))],
        compiler_params=pltpu.CompilerParams(vmem_limit_bytes=16 * 1024 * 1024),
        name="memory",
    )(matrix, norm, top, hidden_in)


def local(
    hidden,
    norm_gains,
    w_query,
    w_key,
    w_value,
    w_outgate,
    w_input_gate,
    w_forget_gate,
    forget_bias,
    w_mix_out,
    state_matrix,
    state_norm,
    state_max,
    routes,
    route_scores,
    expert_gate,
    expert_up,
    expert_down,
    dense_gate,
    dense_up,
    dense_down,
    dense_mix,
):
    new_hidden, matrix, norm, top = whole(
        hidden, norm_gains, dense_mix.reshape(1, -1), routes.T, route_scores.T,
        w_input_gate.T, w_forget_gate.T, forget_bias.reshape(1, -1), state_max.T, state_norm,
        w_query, w_key, w_value, w_outgate, w_mix_out, state_matrix.reshape(64, 128, 128),
        expert_gate.reshape(4, CH, -1), expert_up.reshape(4, CH, -1), expert_down[0],
        dense_gate.T, dense_up.T, dense_down,
    )
    new_norm, new_top, new_hidden, new_matrix = memory(matrix, norm, top, new_hidden)
    return (new_hidden, new_matrix, new_norm, new_top.T)


def solution(mesh):
    placed = (
        P("ep", None),
        P(),
        P(None, "tp"),
        P(None, "tp"),
        P(None, "tp"),
        P(None, "tp"),
        P(),
        P(),
        P(),
        P("tp", None),
        P("ep", "tp", None, None),
        P("ep", "tp", None),
        P("ep", "tp"),
        P("ep", None),
        P("ep", None),
        P("ep", None, "tp"),
        P("ep", None, "tp"),
        P("ep", "tp", None),
        P("tp", "ep"),
        P("tp", "ep"),
        P("ep", "tp"),
        P(),
    )
    return jax.shard_map(
        local,
        mesh=mesh,
        in_specs=placed,
        out_specs=(P("ep", "tp"), P("ep", "tp", None, None), P("ep", "tp", None), P("ep", "tp")),
        check_vma=False,
    )
```

```python
import jax
import jax.numpy as jnp
from jax import lax
from jax.experimental import pallas as pl
from jax.experimental.pallas import tpu as pltpu
from jax.sharding import PartitionSpec as P

EPS = 1e-06
MESH = pl.DeviceIdType.MESH
BF = jnp.bfloat16
F32 = jnp.float32
I32 = jnp.int32
CHIP_STEPS = sorted(
    ((dz, dy) for dz in range(4) for dy in range(4) if dz or dy),
    key=lambda s: -(min(s[0], 4 - s[0]) + min(s[1], 4 - s[1])),
)
EARLY = 7
PIECES = ((0, 96), (96, 80))
CH = 512


def dot(a, b):
    return jnp.dot(a, b, preferred_element_type=F32)


def iota(shape, dim):
    return lax.broadcasted_iota(I32, shape, dim)


def one_hot(columns, rows, target):
    return (iota((rows, columns), 1) == target(iota((rows, columns), 0))).astype(BF)


def stacked(ref):
    return jnp.concatenate([ref[:, q * CH : (q + 1) * CH] for q in range(4)], axis=0)


def row_total(values):
    part = jnp.sum(values, axis=1, keepdims=True)
    total = part[0:8] + part[8:16] + part[16:24] + part[24:32]
    return jnp.concatenate([total] * 4, axis=0)


def silu(t):
    return t / (1.0 + jnp.exp(-t))


def whole_kernel(
    hidden_h, gains_h, mix_h, routes_h, scores_h, w_in_h, w_fg_h, bias_h, smax_h, snorm_h,
    wq_h, wk_h, wv_h, wo_h, wm_h, st_h, eg, eu, ed, dg, du, dd,
    out, matrix, norm_out, max_out,
    hidden, gains, mix, routes, scores, w_in, w_fg, bias, smax, snorm,
    wq, wk, wv, wo, wm, st, numer,
    wg, wu, wd, gbuf, ubuf, dbuf,
    bsend, brecv, hperm, nall, tok, osend, orecv, rsend, rrecv, dsend, drecv, dsum,
    msend, mrecv, fsend, frecv,
    pm, pmi, pd, pdi, gk, xs, xd, ys, yd, hexp, hden, resid_s, mixg_s, share_s,
    load_sem, b_sem, n_sem, t_sem, o_sem, r_sem, d_sem, m_sem, f_sem,
    gs_sem, gr_sem, us_sem, ur_sem, ds_sem, dr_sem,
):
    x = lax.axis_index("tp")
    ep = lax.axis_index("ep")
    c = ep % 2
    y = (ep // 2) % 4
    z = ep // 8
    p = ep // 2
    mate = p * 2 + (1 - c)
    left, right, far = (x + 3) % 4, (x + 1) % 4, (x + 2) % 4

    z_at = [((z + d) % 4) * 8 for d in range(4)]
    y_at = [((y + d) % 4) * 2 for d in range(4)]
    core_at = [c, 1 - c]
    places = [((z + dz) % 4) * 4 + (y + dy) % 4 for dz, dy in CHIP_STEPS]
    chips = [z_at[dz] + y_at[dy] for dz, dy in CHIP_STEPS]
    peers = [p * 2 + core_at[1]]
    for n, base in enumerate(chips):
        peers += [base + core_at[n % 2], base + core_at[1 - n % 2]]

    def remote(src, dst, ssem, rsem, to_ep, to_x):
        return pltpu.make_async_remote_copy(
            src_ref=src, dst_ref=dst, send_sem=ssem, recv_sem=rsem,
            device_id=(to_ep, to_x), device_id_type=MESH,
        )

    def landed(ref, sem):
        pltpu.make_async_copy(ref, ref, sem).wait()

    barrier = pltpu.get_barrier_semaphore()

    loads = {
        name: pltpu.make_async_copy(src, dst, load_sem.at[n])
        for n, (name, src, dst) in enumerate(
            [
                ("hidden", hidden_h, hidden), ("gains", gains_h, gains),
                ("wq", wq_h, wq), ("wk", wk_h, wk), ("w_in", w_in_h, w_in), ("w_fg", w_fg_h, w_fg),
                ("bias", bias_h, bias), ("smax", smax_h, smax), ("wv", wv_h, wv), ("wo", wo_h, wo),
                ("gate", dg, gbuf.at[c, x]), ("st0", st_h.at[pl.ds(0, 32)], st.at[pl.ds(0, 32)]),
                ("st1", st_h.at[pl.ds(32, 32)], st.at[pl.ds(32, 32)]), ("snorm", snorm_h, snorm), ("wm", wm_h, wm),
                ("up", du, ubuf.at[c, x]), ("down", dd, dbuf.at[c, x]), ("mix", mix_h, mix),
                ("routes", routes_h, routes), ("scores", scores_h, scores),
                ("eg", eg, wg), ("eu", eu, wu), ("ed", ed, wd),
            ]
        )
    }
    for name in ("hidden", "gains", "wq", "wk"):
        loads[name].start()
    for d in (2, 1, 3):
        pl.semaphore_signal(barrier, inc=1, device_id=(ep, (x + d) % 4), device_id_type=MESH)
    for peer in peers:
        pl.semaphore_signal(barrier, inc=1, device_id=(peer, x), device_id_type=MESH)
    for name, load in loads.items():
        if name not in ("hidden", "gains", "wq", "wk"):
            load.start()

    def first_round(weight, part):
        buf, ssem, rsem = weight
        copies = []
        for piece, to in ((0, right), (1, left)) if part == 0 else ((1, right), (0, left)):
            block = buf.at[c, x, pl.ds(*PIECES[piece])]
            n = 2 * part + piece
            copies.append(remote(block, block, ssem.at[n], rsem.at[n], ep, to))
        if part == 1:
            block = buf.at[c, x]
            copies.append(remote(block, block, ssem.at[6], rsem.at[6], mate, x))
        for copy in copies:
            copy.start()
        return copies

    def second_round(weight):
        buf, ssem, rsem = weight
        copies = []
        for piece, near, onward in ((0, left, right), (1, right, left)):
            block = buf.at[c, near, pl.ds(*PIECES[piece])]
            landed(block, rsem.at[piece])
            copies.append(remote(block, block, ssem.at[4 + piece], rsem.at[4 + piece], ep, onward))
            copies[-1].start()
        return copies

    def near_to_mate(weight):
        buf, ssem, rsem = weight
        copies = []
        for piece, n, near in ((1, 7, left), (0, 8, right)):
            landed(buf.at[c, near, pl.ds(*PIECES[piece])], rsem.at[2 + piece])
            block = buf.at[c, near]
            copies.append(remote(block, block, ssem.at[n], rsem.at[n], mate, x))
            copies[-1].start()
        return copies

    def far_to_mate(weight):
        buf, ssem, rsem = weight
        copies = []
        for piece in range(2):
            block = buf.at[c, far, pl.ds(*PIECES[piece])]
            landed(block, rsem.at[4 + piece])
            copies.append(remote(block, block, ssem.at[9 + piece], rsem.at[9 + piece], mate, x))
            copies[-1].start()
        return copies

    def from_mate(weight):
        buf, _, rsem = weight
        for n, place in ((6, x), (7, left), (8, right)):
            landed(buf.at[1 - c, place], rsem.at[n])
        for piece in range(2):
            landed(buf.at[1 - c, far, pl.ds(*PIECES[piece])], rsem.at[9 + piece])

    gate_w = (gbuf, gs_sem, gr_sem)
    up_w = (ubuf, us_sem, ur_sem)
    down_w = (dbuf, ds_sem, dr_sem)

    loads["hidden"].wait()
    start_f = hidden[...].astype(F32)
    start_scale = lax.rsqrt(jnp.sum(start_f * start_f, axis=1, keepdims=True) / 2048.0 + EPS)
    loads["gains"].wait()
    normed_in = (start_f * start_scale * gains[0:1, :]).astype(BF)
    same = iota((32, 32), 0) == iota((32, 32), 1)

    def as_column(row):
        return jnp.sum(jnp.where(same, jnp.broadcast_to(row, (32, 32)), 0.0), axis=1, keepdims=True)

    def as_row(column):
        return jnp.sum(jnp.where(same, jnp.broadcast_to(column, (32, 32)), 0.0), axis=0, keepdims=True)

    def along(a, b):
        return lax.dot_general(a, b, (((1,), (1,)), ((), ())), preferred_element_type=F32)

    loads["wq"].wait()
    loads["wk"].wait()
    query = dot(normed_in, wq[...]).astype(BF)
    keys = dot(normed_in, wk[...]).astype(BF).astype(F32) * 128.0 ** (-0.5)
    for name in ("w_in", "w_fg", "bias", "smax"):
        loads[name].wait()
    gate_in = along(normed_in, w_in[...])
    forget = along(normed_in, w_fg[...]) + bias[...]
    forget = jnp.minimum(forget, 0.0) - jnp.log(1.0 + jnp.exp(-jnp.abs(forget)))
    head8 = iota((32, 8), 1)
    keeps, writes, floors = [], [], []
    for h in range(2):
        mine = head8 == 2 * x + h
        in_gate = jnp.sum(jnp.where(mine, gate_in, 0.0), axis=1, keepdims=True)
        carried = jnp.sum(jnp.where(mine, forget, 0.0), axis=1, keepdims=True) + as_column(smax[h : h + 1, :])
        new_max = jnp.maximum(carried, in_gate)
        keeps.append(jnp.exp(carried - new_max))
        writes.append(jnp.exp(in_gate - new_max))
        floors.append(jnp.exp(-new_max))
        max_out[h : h + 1, :] = as_row(new_max)
    loads["wv"].wait()
    loads["wo"].wait()
    value = dot(normed_in, wv[...]).astype(BF).astype(F32)
    out_gate = dot(normed_in, wo[...]).astype(BF).astype(F32)

    pl.semaphore_wait(barrier, 34)
    loads["gate"].wait()
    weight_out = first_round(gate_w, 0)

    eye = same.astype(BF)
    queries_t = [
        lax.dot_general(
            query[:, h * 128 : (h + 1) * 128], eye, (((0,), (0,)), ((), ())), preferred_element_type=F32
        ).astype(BF)
        for h in range(2)
    ]
    for half in range(2):
        loads[("st0", "st1")[half]].wait()
        for h in range(2):
            for s in range(16 * half, 16 * half + 16, 2):
                wide = dot(queries_t[h], (iota((32, 256), 0) == s + (iota((32, 256), 1) >> 7)).astype(BF))
                numer[h, s : s + 1, :] = jnp.sum(wide[:, 0:128] * st[s * 2 + h], axis=0, keepdims=True)
                numer[h, s + 1 : s + 2, :] = jnp.sum(
                    wide[:, 128:256] * st[s * 2 + 2 + h], axis=0, keepdims=True
                )
    loads["snorm"].wait()
    mixed, written_t = [], []
    for h in range(2):
        lanes = slice(h * 128, (h + 1) * 128)
        q = query[:, lanes].astype(F32)
        written = writes[h] * keys[:, lanes]
        new_norm = keeps[h] * snorm[:, h, :] + written
        top = keeps[h] * numer[h] + jnp.sum(q * written, axis=1, keepdims=True) * value[:, lanes]
        denom = jnp.sum(q * new_norm, axis=1, keepdims=True)
        read = top / jnp.maximum(jnp.abs(denom), floors[h])
        mixed.append((read / (1.0 + jnp.exp(-out_gate[:, lanes]))).astype(BF))
        written_t.append(jnp.transpose(written))
        norm_out[:, h, :] = new_norm
    loads["wm"].wait()
    share = [
        (dot(mixed[0], wm[0:128, q * CH : (q + 1) * CH]) + dot(mixed[1], wm[128:256, q * CH : (q + 1) * CH])).astype(BF)
        for q in range(4)
    ]

    order = one_hot(128, 128, lambda r: ((r >> 3) & 3) * 32 + (r >> 5) * 8 + (r & 7))
    bsend[...] = dot(order, jnp.concatenate(share, axis=0)).astype(BF).reshape(4, 32, CH)
    brecv[x] = bsend[x]
    branch_out = []
    for d in (2, 1, 3):
        to = (x + d) % 4
        branch_out.append(remote(bsend.at[to], brecv.at[x], b_sem.at[0], b_sem.at[1], ep, to))
        branch_out[-1].start()

    weight_out += first_round(gate_w, 1)
    hperm[...] = dot(order, stacked(hidden)).reshape(4, 32, CH)

    for name in ("mix", "routes", "scores"):
        loads[name].wait()
    expert0, expert1 = as_column(routes[0:1, :].astype(F32)), as_column(routes[1:2, :].astype(F32))
    lane32 = iota((32, 32), 1)
    lane32_f = lane32.astype(F32)
    hot0 = (lane32_f == expert0).astype(F32)
    hot1 = (lane32_f == expert1).astype(F32)
    earlier = (iota((32, 32), 0) > lane32).astype(BF)
    before = dot(earlier, (hot0 + hot1).astype(BF))
    score0, score1 = as_column(scores[0:1, :]), as_column(scores[1:2, :])
    whole = score0 + score1

    def by_piece(column, step):
        return jnp.concatenate(
            [column[xx * 8 : xx * 8 + 8] + q * step for xx in range(4) for q in range(4)], axis=0
        )

    for k, (expert, hot, score) in enumerate(((expert0, hot0, score0), (expert1, hot1, score1))):
        rank = jnp.sum(hot * before, axis=1, keepdims=True)
        place = by_piece((expert * 16.0 + rank).astype(I32), 4)
        gk[k] = (iota((128, 512), 1) == place).astype(BF)
        share_s[k] = jnp.broadcast_to(by_piece(score / whole, 0.0), (128, 128))
    pm[...] = one_hot(512, 512, lambda r: ((r >> 2) & 31) * 16 + (r >> 7) * 4 + (r & 3))
    pmi[...] = one_hot(512, 512, lambda r: ((r >> 2) & 3) * 128 + (r >> 4) * 4 + (r & 3))
    pd[...] = one_hot(512, 512, lambda r: ((r >> 3) & 15) * 32 + (r >> 7) * 8 + (r & 7))
    pdi[...] = one_hot(256, 256, lambda r: ((r >> 3) & 1) * 128 + (r >> 4) * 8 + (r & 7))

    def gain(k):
        return jnp.concatenate(
            [jnp.broadcast_to(gains[k : k + 1, q * CH : (q + 1) * CH], (8, CH)) for q in range(4)],
            axis=0,
        )

    mix_rows = jnp.concatenate(
        [jnp.broadcast_to(mix[0:1, q * CH : (q + 1) * CH], (8, CH)) for q in range(4)], axis=0
    )

    for h in range(2):
        for s in range(32):
            matrix[s, h] = (
                keeps[h][s : s + 1, :] * st[s * 2 + h]
                + written_t[h][:, s : s + 1] * value[s : s + 1, h * 128 : (h + 1) * 128]
            )

    landed(brecv.at[pl.ds(0, 3)], b_sem.at[1])
    branch = brecv[0].astype(F32) + brecv[1].astype(F32) + brecv[2].astype(F32) + brecv[3].astype(F32)
    branch = branch.astype(BF).astype(F32)
    residual_f = hperm[x] + gain(1) * branch * lax.rsqrt(row_total(branch * branch) / 2048.0 + EPS)
    scale_two = lax.rsqrt(row_total(residual_f * residual_f) / 2048.0 + EPS)
    normed = (residual_f * scale_two * gain(2)).astype(BF)
    nall[x] = normed
    tok[p] = normed

    token_out = []
    for d in (2, 1, 3):
        to = (x + d) % 4
        token_out.append(remote(nall.at[x], nall.at[x], n_sem.at[0], n_sem.at[1], ep, to))
        token_out[-1].start()

    for chip in chips[:EARLY]:
        remote(nall.at[x], tok.at[p], t_sem.at[0], t_sem.at[1], chip + c, x).start()
    loads["up"].wait()
    loads["down"].wait()
    resid_s[...] = residual_f.astype(BF).astype(F32)
    mix_dot = scale_two * row_total(residual_f * gain(2) * mix_rows)
    mixg_s[...] = jnp.broadcast_to(1.0 / (1.0 + jnp.exp(-mix_dot)), (32, 128))

    landed(nall.at[pl.ds(0, 3)], n_sem.at[1])
    chosen = gk[0] + gk[1]
    rows = lax.dot_general(
        chosen, nall[...].reshape(128, CH), (((0,), (0,)), ((), ())), preferred_element_type=F32
    )
    osend[...] = rows.astype(BF).reshape(32, 16, CH)
    orecv[ep] = osend[ep]

    for peer in peers:
        remote(osend.at[peer], orecv.at[ep], o_sem.at[0], o_sem.at[1], peer, x).start()
    weight_out += first_round(up_w, 0) + first_round(up_w, 1)
    weight_out += second_round(gate_w)
    for chip in chips[EARLY:]:
        remote(nall.at[x], tok.at[p], t_sem.at[0], t_sem.at[1], chip + c, x).start()
    weight_out += near_to_mate(gate_w)
    weight_out += second_round(up_w)
    weight_out += first_round(down_w, 0) + first_round(down_w, 1)
    weight_out += near_to_mate(up_w)

    landed(orecv.at[pl.ds(0, 31)], o_sem.at[1])
    xs[...] = dot(pm[...], orecv[...].reshape(512, CH)).astype(BF).reshape(4, 128, CH)
    loads["eg"].wait()
    loads["eu"].wait()
    gate_pre = dot(xs[0], wg[0])
    up_pre = dot(xs[0], wu[0])
    for q in range(1, 4):
        gate_pre += dot(xs[q], wg[q])
        up_pre += dot(xs[q], wu[q])
    hexp[...] = (silu(gate_pre) * up_pre).astype(BF)
    weight_out += far_to_mate(gate_w)
    loads["ed"].wait()
    for q in range(4):
        ys[q * 128 : (q + 1) * 128] = dot(hexp[...], wd[:, q * CH : (q + 1) * CH]).astype(BF)
    rsend[...] = dot(pmi[...], ys[...]).astype(BF).reshape(32, 16, CH)
    rrecv[ep] = rsend[ep]

    for peer in peers:
        remote(rsend.at[peer], rrecv.at[ep], r_sem.at[0], r_sem.at[1], peer, x).start()

    weight_out += far_to_mate(up_w)
    weight_out += second_round(down_w)

    landed(tok.at[pl.ds(0, 15)], t_sem.at[1])
    xd[...] = dot(pd[...], tok[...].reshape(512, CH)).astype(BF).reshape(4, 128, CH)
    weight_out += near_to_mate(down_w)
    from_mate(gate_w)
    from_mate(up_w)
    for core in range(2):
        pre_gate = along(xd[0], gbuf[core, 0])
        pre_up = along(xd[0], ubuf[core, 0])
        for q in range(1, 4):
            pre_gate += along(xd[q], gbuf[core, q])
            pre_up += along(xd[q], ubuf[core, q])
        hden[core] = (silu(pre_gate) * pre_up).astype(BF)

    def dense_half(half):
        for n in (2 * half, 2 * half + 1):
            yd[n * 128 : (n + 1) * 128] = (
                dot(hden[0], dbuf[0, quarters[n]]) + dot(hden[1], dbuf[1, quarters[n]])
            ).astype(BF)
        rows = dot(pdi[...], yd[half * 256 : (half + 1) * 256])
        dsend[half] = rows.astype(BF).reshape(16, 16, CH)
        drecv[half, p] = dsend[half, p]
        for chip, place in zip(chips, places):
            remote(
                dsend.at[half, place], drecv.at[half, p],
                d_sem.at[2 * half], d_sem.at[2 * half + 1], chip + c, x,
            ).start()

    quarters = (x, left, right, far)
    landed(dbuf.at[1 - c, x], dr_sem.at[6])
    landed(dbuf.at[1 - c, left], dr_sem.at[7])
    dense_half(0)
    weight_out += far_to_mate(down_w)
    landed(dbuf.at[1 - c, right], dr_sem.at[8])
    for piece in range(2):
        landed(dbuf.at[1 - c, far, pl.ds(*PIECES[piece])], dr_sem.at[9 + piece])
    dense_half(1)

    landed(rrecv.at[pl.ds(0, 31)], r_sem.at[1])
    back = rrecv[...].reshape(512, CH)
    moe = share_s[0][:, 0:1] * dot(gk[0], back) + share_s[1][:, 0:1] * dot(gk[1], back)
    msend[...] = moe.astype(BF).reshape(4, 32, CH)
    mrecv[x] = msend[x]
    moe_out = []
    for d in (2, 1, 3):
        to = (x + d) % 4
        moe_out.append(remote(msend.at[to], mrecv.at[x], m_sem.at[0], m_sem.at[1], ep, to))
        moe_out[-1].start()

    for half in range(2):
        landed(drecv.at[half, pl.ds(0, 15)], d_sem.at[2 * half + 1])
        total = drecv[half, 0].astype(F32)
        for n in range(1, 16):
            total += drecv[half, n].astype(F32)
        dsum[quarters[2 * half]] = total[0:8]
        dsum[quarters[2 * half + 1]] = total[8:16]
    dense = dsum[...].reshape(32, CH)
    landed(mrecv.at[pl.ds(0, 3)], m_sem.at[1])
    ffn = mrecv[0].astype(F32) + mrecv[1].astype(F32) + mrecv[2].astype(F32) + mrecv[3].astype(F32)
    ffn += mixg_s[:, 0:1] * dense
    scale_ffn = lax.rsqrt(row_total(ffn * ffn) / 2048.0 + EPS)
    fsend[...] = (resid_s[...] + gain(3) * ffn * scale_ffn).reshape(4, 8, CH)
    frecv[x] = fsend[x]
    last_out = []
    for d in (2, 1, 3):
        to = (x + d) % 4
        last_out.append(remote(fsend.at[to], frecv.at[x], f_sem.at[0], f_sem.at[1], ep, to))
        last_out[-1].start()

    for copy in weight_out:
        copy.wait_send()
    landed(bsend.at[pl.ds(0, 3)], b_sem.at[0])
    landed(nall.at[pl.ds(0, 3)], n_sem.at[0])
    landed(tok.at[pl.ds(0, 15)], t_sem.at[0])
    landed(osend.at[pl.ds(0, 31)], o_sem.at[0])
    landed(rsend.at[pl.ds(0, 31)], r_sem.at[0])
    landed(dsend.at[0, pl.ds(0, 15)], d_sem.at[0])
    landed(dsend.at[1, pl.ds(0, 15)], d_sem.at[2])
    landed(msend.at[pl.ds(0, 3)], m_sem.at[0])
    landed(frecv.at[pl.ds(0, 3)], f_sem.at[1])
    out[...] = frecv[...].reshape(32, CH).astype(BF)
    landed(fsend.at[pl.ds(0, 3)], f_sem.at[0])


def whole(*arrays):
    V = pltpu.VMEM
    dma = pltpu.SemaphoreType.DMA
    vm = pl.BlockSpec(memory_space=pltpu.VMEM)
    hb = pl.BlockSpec(memory_space=pltpu.HBM)
    return pl.pallas_call(
        whole_kernel,
        out_shape=(
            V((32, CH), BF), V((32, 2, 128, 128), F32), V((32, 2, 128), F32), V((2, 32), F32),
        ),
        in_specs=[hb] * len(arrays),
        out_specs=(vm,) * 4,
        scratch_shapes=[
            V((32, 2048), BF), V((4, 2048), F32), V((1, 2048), F32), V((2, 32), I32), V((2, 32), F32),
            V((8, 2048), BF), V((8, 2048), BF), V((1, 8), F32), V((2, 32), F32), V((32, 2, 128), F32),
            V((2048, 256), BF), V((2048, 256), BF), V((2048, 256), BF), V((2048, 256), BF),
            V((256, 2048), BF), V((64, 128, 128), F32), V((2, 32, 128), F32),
            V((4, 512, 896), BF), V((4, 512, 896), BF), V((896, 2048), BF),
            V((2, 4, 176, 512), BF), V((2, 4, 176, 512), BF), V((2, 4, 176, 512), BF),
            V((4, 32, CH), BF), V((4, 32, CH), BF), V((4, 32, CH), F32), V((4, 32, CH), BF),
            V((16, 32, CH), BF),
            V((32, 16, CH), BF), V((32, 16, CH), BF), V((32, 16, CH), BF), V((32, 16, CH), BF),
            V((2, 16, 16, CH), BF), V((2, 16, 16, CH), BF), V((4, 8, CH), F32),
            V((4, 32, CH), BF), V((4, 32, CH), BF), V((4, 8, CH), F32), V((4, 8, CH), F32),
            V((512, 512), BF), V((512, 512), BF), V((512, 512), BF), V((256, 256), BF),
            V((2, 128, 512), BF), V((4, 128, CH), BF), V((4, 128, CH), BF),
            V((512, CH), BF), V((512, CH), BF), V((128, 896), BF), V((2, 128, 176), BF),
            V((32, CH), F32), V((32, 128), F32), V((2, 128, 128), F32),
            dma((23,)), dma((2,)), dma((2,)), dma((2,)), dma((2,)), dma((2,)), dma((4,)),
            dma((2,)), dma((2,)),
            dma((11,)), dma((11,)), dma((11,)), dma((11,)), dma((11,)), dma((11,)),
        ],
        compiler_params=pltpu.CompilerParams(
            collective_id=0, has_side_effects=True, vmem_limit_bytes=44 * 1024 * 1024
        ),
        name="whole",
    )(*(pltpu.with_memory_space_constraint(a, pltpu.HBM) for a in arrays))


def memory_kernel(matrix, norm, top, last, matrix_h, norm_h, top_h, last_h, sem):
    stores = [
        pltpu.make_async_copy(matrix.at[pl.ds(n * 4, 4)], matrix_h.at[pl.ds(n * 4, 4)], sem.at[n])
        for n in range(8)
    ]
    for n, (src, dst) in enumerate(((norm, norm_h), (top, top_h), (last, last_h))):
        stores.append(pltpu.make_async_copy(src, dst, sem.at[8 + n]))
    for store in stores:
        store.start()
    for store in stores:
        store.wait()


def memory(matrix, norm, top, last):
    arrays = (matrix, norm, top, last)
    return pl.pallas_call(
        memory_kernel,
        out_shape=tuple(pltpu.HBM(a.shape, a.dtype) for a in arrays),
        in_specs=[pl.BlockSpec(memory_space=pltpu.VMEM)] * 4,
        out_specs=(pl.BlockSpec(memory_space=pltpu.HBM),) * 4,
        scratch_shapes=[pltpu.SemaphoreType.DMA((11,))],
        compiler_params=pltpu.CompilerParams(vmem_limit_bytes=16 * 1024 * 1024),
        name="memory",
    )(*arrays)


def local(
    hidden,
    norm_gains,
    w_query,
    w_key,
    w_value,
    w_outgate,
    w_input_gate,
    w_forget_gate,
    forget_bias,
    w_mix_out,
    state_matrix,
    state_norm,
    state_max,
    routes,
    route_scores,
    expert_gate,
    expert_up,
    expert_down,
    dense_gate,
    dense_up,
    dense_down,
    dense_mix,
):
    new_hidden, matrix, norm, top = whole(
        hidden, norm_gains, dense_mix.reshape(1, -1), routes.T, route_scores.T,
        w_input_gate.T, w_forget_gate.T, forget_bias.reshape(1, -1), state_max.T, state_norm,
        w_query, w_key, w_value, w_outgate, w_mix_out, state_matrix.reshape(64, 128, 128),
        expert_gate.reshape(4, CH, -1), expert_up.reshape(4, CH, -1), expert_down[0],
        dense_gate.T, dense_up.T, dense_down,
    )
    new_matrix, new_norm, new_top, new_hidden = memory(matrix, norm, top, new_hidden)
    return (new_hidden, new_matrix, new_norm, new_top.T)


def solution(mesh):
    placed = (
        P("ep", None),
        P(),
        P(None, "tp"),
        P(None, "tp"),
        P(None, "tp"),
        P(None, "tp"),
        P(),
        P(),
        P(),
        P("tp", None),
        P("ep", "tp", None, None),
        P("ep", "tp", None),
        P("ep", "tp"),
        P("ep", None),
        P("ep", None),
        P("ep", None, "tp"),
        P("ep", None, "tp"),
        P("ep", "tp", None),
        P("tp", "ep"),
        P("tp", "ep"),
        P("ep", "tp"),
        P(),
    )
    return jax.shard_map(
        local,
        mesh=mesh,
        in_specs=placed,
        out_specs=(P("ep", "tp"), P("ep", "tp", None, None), P("ep", "tp", None), P("ep", "tp")),
        check_vma=False,
    )
```

```python
import jax
import jax.numpy as jnp
from jax import lax
from jax.experimental import pallas as pl
from jax.experimental.pallas import tpu as pltpu
from jax.sharding import PartitionSpec as P

EPS = 1e-06
MESH = pl.DeviceIdType.MESH
BF = jnp.bfloat16
F32 = jnp.float32
I32 = jnp.int32
CHIP_STEPS = sorted(
    ((dz, dy) for dz in range(4) for dy in range(4) if dz or dy),
    key=lambda s: -(min(s[0], 4 - s[0]) + min(s[1], 4 - s[1])),
)
EARLY = 7
PIECES = ((0, 96), (96, 80))
CH = 512


def dot(a, b):
    return jnp.dot(a, b, preferred_element_type=F32)


def iota(shape, dim):
    return lax.broadcasted_iota(I32, shape, dim)


def one_hot(columns, rows, target):
    return (iota((rows, columns), 1) == target(iota((rows, columns), 0))).astype(BF)


def stacked(ref):
    return jnp.concatenate([ref[:, q * CH : (q + 1) * CH] for q in range(4)], axis=0)


def row_total(values):
    part = jnp.sum(values, axis=1, keepdims=True)
    total = part[0:8] + part[8:16] + part[16:24] + part[24:32]
    return jnp.concatenate([total] * 4, axis=0)


def silu(t):
    return t / (1.0 + jnp.exp(-t))


def whole_kernel(
    hidden_h, gains_h, mix_h, routes_h, scores_h, w_in_h, w_fg_h, bias_h, smax_h, snorm_h,
    wq_h, wk_h, wv_h, wo_h, wm_h, st_h, eg, eu, ed, dg, du, dd,
    out, matrix, norm_out, max_out,
    hidden, gains, mix, routes, scores, w_in, w_fg, bias, smax, snorm,
    wq, wk, wv, wo, wm, st, numer,
    wg, wu, wd, gbuf, ubuf, dbuf,
    bsend, brecv, hperm, nall, tok, osend, orecv, rsend, rrecv, dsend, drecv, dsum,
    msend, mrecv, fsend, frecv,
    pm, pmi, pd, chosen, gk, xs, xd, ys, hexp, hden, resid_s, mixg_s, share_s,
    load_sem, b_sem, n_sem, t_sem, o_sem, r_sem, d_sem, m_sem, f_sem,
    gs_sem, gr_sem, us_sem, ur_sem, ds_sem, dr_sem,
):
    x = lax.axis_index("tp")
    ep = lax.axis_index("ep")
    c = ep % 2
    y = (ep // 2) % 4
    z = ep // 8
    p = ep // 2
    mate = p * 2 + (1 - c)
    left, right, far = (x + 3) % 4, (x + 1) % 4, (x + 2) % 4

    z_at = [((z + d) % 4) * 8 for d in range(4)]
    y_at = [((y + d) % 4) * 2 for d in range(4)]
    core_at = [c, 1 - c]
    places = [((z + dz) % 4) * 4 + (y + dy) % 4 for dz, dy in CHIP_STEPS]
    chips = [z_at[dz] + y_at[dy] for dz, dy in CHIP_STEPS]
    peers = [p * 2 + core_at[1]]
    for n, base in enumerate(chips):
        peers += [base + core_at[n % 2], base + core_at[1 - n % 2]]

    def remote(src, dst, ssem, rsem, to_ep, to_x):
        return pltpu.make_async_remote_copy(
            src_ref=src, dst_ref=dst, send_sem=ssem, recv_sem=rsem,
            device_id=(to_ep, to_x), device_id_type=MESH,
        )

    def landed(ref, sem):
        pltpu.make_async_copy(ref, ref, sem).wait()

    barrier = pltpu.get_barrier_semaphore()

    loads = {
        name: pltpu.make_async_copy(src, dst, load_sem.at[n])
        for n, (name, src, dst) in enumerate(
            [
                ("hidden", hidden_h, hidden), ("gains", gains_h, gains),
                ("wq", wq_h, wq), ("wk", wk_h, wk), ("w_in", w_in_h, w_in), ("w_fg", w_fg_h, w_fg),
                ("bias", bias_h, bias), ("smax", smax_h, smax), ("wv", wv_h, wv), ("wo", wo_h, wo),
                ("gate", dg, gbuf.at[c, x]), ("st0", st_h.at[pl.ds(0, 32)], st.at[pl.ds(0, 32)]),
                ("st1", st_h.at[pl.ds(32, 32)], st.at[pl.ds(32, 32)]), ("snorm", snorm_h, snorm), ("wm", wm_h, wm),
                ("up", du, ubuf.at[c, x]), ("down", dd, dbuf.at[c, x]), ("mix", mix_h, mix),
                ("routes", routes_h, routes), ("scores", scores_h, scores),
                ("eg", eg, wg), ("eu", eu, wu), ("ed", ed, wd),
            ]
        )
    }
    for name in ("hidden", "gains", "wq", "wk"):
        loads[name].start()
    for d in (2, 1, 3):
        pl.semaphore_signal(barrier, inc=1, device_id=(ep, (x + d) % 4), device_id_type=MESH)
    for peer in peers:
        pl.semaphore_signal(barrier, inc=1, device_id=(peer, x), device_id_type=MESH)
    for name, load in loads.items():
        if name not in ("hidden", "gains", "wq", "wk"):
            load.start()

    def first_round(weight, part):
        buf, ssem, rsem = weight
        copies = []
        for piece, to in ((0, right), (1, left)) if part == 0 else ((1, right), (0, left)):
            block = buf.at[c, x, pl.ds(*PIECES[piece])]
            n = 2 * part + piece
            copies.append(remote(block, block, ssem.at[n], rsem.at[n], ep, to))
        if part == 1:
            block = buf.at[c, x]
            copies.append(remote(block, block, ssem.at[6], rsem.at[6], mate, x))
        for copy in copies:
            copy.start()
        return copies

    def second_round(weight):
        buf, ssem, rsem = weight
        copies = []
        for piece, near, onward in ((0, left, right), (1, right, left)):
            block = buf.at[c, near, pl.ds(*PIECES[piece])]
            landed(block, rsem.at[piece])
            copies.append(remote(block, block, ssem.at[4 + piece], rsem.at[4 + piece], ep, onward))
            copies[-1].start()
        return copies

    def near_to_mate(weight):
        buf, ssem, rsem = weight
        copies = []
        for piece, n, near in ((1, 7, left), (0, 8, right)):
            landed(buf.at[c, near, pl.ds(*PIECES[piece])], rsem.at[2 + piece])
            block = buf.at[c, near]
            copies.append(remote(block, block, ssem.at[n], rsem.at[n], mate, x))
            copies[-1].start()
        return copies

    def far_to_mate(weight):
        buf, ssem, rsem = weight
        copies = []
        for piece in range(2):
            block = buf.at[c, far, pl.ds(*PIECES[piece])]
            landed(block, rsem.at[4 + piece])
            copies.append(remote(block, block, ssem.at[9 + piece], rsem.at[9 + piece], mate, x))
            copies[-1].start()
        return copies

    def from_mate(weight):
        buf, _, rsem = weight
        for n, place in ((6, x), (7, left), (8, right)):
            landed(buf.at[1 - c, place], rsem.at[n])
        for piece in range(2):
            landed(buf.at[1 - c, far, pl.ds(*PIECES[piece])], rsem.at[9 + piece])

    gate_w = (gbuf, gs_sem, gr_sem)
    up_w = (ubuf, us_sem, ur_sem)
    down_w = (dbuf, ds_sem, dr_sem)

    loads["hidden"].wait()
    start_f = hidden[...].astype(F32)
    start_scale = lax.rsqrt(jnp.sum(start_f * start_f, axis=1, keepdims=True) / 2048.0 + EPS)
    loads["gains"].wait()
    normed_in = (start_f * start_scale * gains[0:1, :]).astype(BF)
    same = iota((32, 32), 0) == iota((32, 32), 1)

    def as_column(row):
        return jnp.sum(jnp.where(same, jnp.broadcast_to(row, (32, 32)), 0.0), axis=1, keepdims=True)

    def as_row(column):
        return jnp.sum(jnp.where(same, jnp.broadcast_to(column, (32, 32)), 0.0), axis=0, keepdims=True)

    def along(a, b):
        return lax.dot_general(a, b, (((1,), (1,)), ((), ())), preferred_element_type=F32)

    loads["wq"].wait()
    loads["wk"].wait()
    query = dot(normed_in, wq[...]).astype(BF)
    keys = dot(normed_in, wk[...]).astype(BF).astype(F32) * 128.0 ** (-0.5)
    for name in ("w_in", "w_fg", "bias", "smax"):
        loads[name].wait()
    gate_in = along(normed_in, w_in[...])
    forget = along(normed_in, w_fg[...]) + bias[...]
    forget = jnp.minimum(forget, 0.0) - jnp.log(1.0 + jnp.exp(-jnp.abs(forget)))
    head8 = iota((32, 8), 1)
    keeps, writes, floors = [], [], []
    for h in range(2):
        mine = head8 == 2 * x + h
        in_gate = jnp.sum(jnp.where(mine, gate_in, 0.0), axis=1, keepdims=True)
        carried = jnp.sum(jnp.where(mine, forget, 0.0), axis=1, keepdims=True) + as_column(smax[h : h + 1, :])
        new_max = jnp.maximum(carried, in_gate)
        keeps.append(jnp.exp(carried - new_max))
        writes.append(jnp.exp(in_gate - new_max))
        floors.append(jnp.exp(-new_max))
        max_out[h : h + 1, :] = as_row(new_max)
    loads["wv"].wait()
    loads["wo"].wait()
    value = dot(normed_in, wv[...]).astype(BF).astype(F32)
    out_gate = dot(normed_in, wo[...]).astype(BF).astype(F32)

    pl.semaphore_wait(barrier, 34)
    loads["gate"].wait()
    weight_out = first_round(gate_w, 0)

    eye = same.astype(BF)
    queries_t = [
        lax.dot_general(
            query[:, h * 128 : (h + 1) * 128], eye, (((0,), (0,)), ((), ())), preferred_element_type=F32
        ).astype(BF)
        for h in range(2)
    ]
    for half in range(2):
        loads[("st0", "st1")[half]].wait()
        for h in range(2):
            for s in range(16 * half, 16 * half + 16, 2):
                wide = dot(queries_t[h], (iota((32, 256), 0) == s + (iota((32, 256), 1) >> 7)).astype(BF))
                numer[h, s : s + 1, :] = jnp.sum(wide[:, 0:128] * st[s * 2 + h], axis=0, keepdims=True)
                numer[h, s + 1 : s + 2, :] = jnp.sum(
                    wide[:, 128:256] * st[s * 2 + 2 + h], axis=0, keepdims=True
                )
    loads["snorm"].wait()
    mixed, written_t = [], []
    for h in range(2):
        lanes = slice(h * 128, (h + 1) * 128)
        q = query[:, lanes].astype(F32)
        written = writes[h] * keys[:, lanes]
        new_norm = keeps[h] * snorm[:, h, :] + written
        top = keeps[h] * numer[h] + jnp.sum(q * written, axis=1, keepdims=True) * value[:, lanes]
        denom = jnp.sum(q * new_norm, axis=1, keepdims=True)
        read = top / jnp.maximum(jnp.abs(denom), floors[h])
        mixed.append((read / (1.0 + jnp.exp(-out_gate[:, lanes]))).astype(BF))
        written_t.append(jnp.transpose(written))
        norm_out[:, h, :] = new_norm
    loads["wm"].wait()
    share = [
        (dot(mixed[0], wm[0:128, q * CH : (q + 1) * CH]) + dot(mixed[1], wm[128:256, q * CH : (q + 1) * CH]))
        for q in range(4)
    ]

    for xx in range(4):
        bsend[xx] = jnp.concatenate([part[xx * 8 : xx * 8 + 8] for part in share], axis=0).astype(BF)
    brecv[x] = bsend[x]
    branch_out = []
    for d in (2, 1, 3):
        to = (x + d) % 4
        branch_out.append(remote(bsend.at[to], brecv.at[x], b_sem.at[0], b_sem.at[1], ep, to))
        branch_out[-1].start()

    weight_out += first_round(gate_w, 1)
    order = one_hot(128, 128, lambda r: ((r >> 3) & 3) * 32 + (r >> 5) * 8 + (r & 7))
    hperm[...] = dot(order, stacked(hidden)).reshape(4, 32, CH)

    for name in ("mix", "routes", "scores"):
        loads[name].wait()
    expert0, expert1 = as_column(routes[0:1, :].astype(F32)), as_column(routes[1:2, :].astype(F32))
    lane32 = iota((32, 32), 1)
    lane32_f = lane32.astype(F32)
    hot0 = (lane32_f == expert0).astype(F32)
    hot1 = (lane32_f == expert1).astype(F32)
    earlier = (iota((32, 32), 0) > lane32).astype(BF)
    before = dot(earlier, (hot0 + hot1).astype(BF))
    score0, score1 = as_column(scores[0:1, :]), as_column(scores[1:2, :])
    whole = score0 + score1

    def by_piece(column, step):
        return jnp.concatenate(
            [column[xx * 8 : xx * 8 + 8] + q * step for xx in range(4) for q in range(4)], axis=0
        )

    for k, (expert, hot, score) in enumerate(((expert0, hot0, score0), (expert1, hot1, score1))):
        rank = jnp.sum(hot * before, axis=1, keepdims=True)
        place = by_piece((expert * 16.0 + rank).astype(I32), 4)
        gk[k] = (iota((128, 512), 1) == place).astype(BF)
        share_s[k] = jnp.broadcast_to(by_piece(score / whole, 0.0), (128, 128))
    chosen[...] = jnp.transpose((gk[0] + gk[1]).astype(F32)).astype(BF)
    pm[...] = one_hot(512, 512, lambda r: ((r >> 2) & 31) * 16 + (r >> 7) * 4 + (r & 3))
    pmi[...] = one_hot(512, 512, lambda r: ((r >> 2) & 3) * 128 + (r >> 4) * 4 + (r & 3))
    pd[...] = one_hot(512, 512, lambda r: ((r >> 3) & 15) * 32 + (r >> 7) * 8 + (r & 7))

    def gain(k):
        return jnp.concatenate(
            [jnp.broadcast_to(gains[k : k + 1, q * CH : (q + 1) * CH], (8, CH)) for q in range(4)],
            axis=0,
        )

    mix_rows = jnp.concatenate(
        [jnp.broadcast_to(mix[0:1, q * CH : (q + 1) * CH], (8, CH)) for q in range(4)], axis=0
    )

    for h in range(2):
        for s in range(32):
            matrix[s, h] = (
                keeps[h][s : s + 1, :] * st[s * 2 + h]
                + written_t[h][:, s : s + 1] * value[s : s + 1, h * 128 : (h + 1) * 128]
            )

    landed(brecv.at[pl.ds(0, 3)], b_sem.at[1])
    branch = brecv[0].astype(F32) + brecv[1].astype(F32) + brecv[2].astype(F32) + brecv[3].astype(F32)
    branch = branch.astype(BF).astype(F32)
    residual_f = hperm[x] + gain(1) * branch * lax.rsqrt(row_total(branch * branch) / 2048.0 + EPS)
    scale_two = lax.rsqrt(row_total(residual_f * residual_f) / 2048.0 + EPS)
    normed = (residual_f * scale_two * gain(2)).astype(BF)
    nall[x] = normed
    tok[p] = normed

    token_out = []
    for d in (2, 1, 3):
        to = (x + d) % 4
        token_out.append(remote(nall.at[x], nall.at[x], n_sem.at[0], n_sem.at[1], ep, to))
        token_out[-1].start()

    for chip in chips[:EARLY]:
        remote(nall.at[x], tok.at[p], t_sem.at[0], t_sem.at[1], chip + c, x).start()
    loads["up"].wait()
    loads["down"].wait()
    resid_s[...] = residual_f.astype(BF).astype(F32)
    mix_dot = scale_two * row_total(residual_f * gain(2) * mix_rows)
    mixg_s[...] = jnp.broadcast_to(1.0 / (1.0 + jnp.exp(-mix_dot)), (32, 128))

    landed(nall.at[pl.ds(0, 3)], n_sem.at[1])
    rows = dot(chosen[...], nall[...].reshape(128, CH))
    osend[...] = rows.astype(BF).reshape(32, 16, CH)
    orecv[ep] = osend[ep]

    for peer in peers:
        remote(osend.at[peer], orecv.at[ep], o_sem.at[0], o_sem.at[1], peer, x).start()
    weight_out += first_round(up_w, 0) + first_round(up_w, 1)
    weight_out += second_round(gate_w)
    for chip in chips[EARLY:]:
        remote(nall.at[x], tok.at[p], t_sem.at[0], t_sem.at[1], chip + c, x).start()
    weight_out += near_to_mate(gate_w)
    weight_out += second_round(up_w)
    weight_out += first_round(down_w, 0) + first_round(down_w, 1)
    weight_out += near_to_mate(up_w)

    landed(orecv.at[pl.ds(0, 31)], o_sem.at[1])
    xs[...] = dot(pm[...], orecv[...].reshape(512, CH)).astype(BF).reshape(4, 128, CH)
    loads["eg"].wait()
    loads["eu"].wait()
    gate_pre = dot(xs[0], wg[0])
    up_pre = dot(xs[0], wu[0])
    for q in range(1, 4):
        gate_pre += dot(xs[q], wg[q])
        up_pre += dot(xs[q], wu[q])
    hexp[...] = (silu(gate_pre) * up_pre).astype(BF)
    weight_out += far_to_mate(gate_w)
    loads["ed"].wait()
    for q in range(4):
        ys[q * 128 : (q + 1) * 128] = dot(hexp[...], wd[:, q * CH : (q + 1) * CH]).astype(BF)
    rsend[...] = dot(pmi[...], ys[...]).astype(BF).reshape(32, 16, CH)
    rrecv[ep] = rsend[ep]

    for peer in peers:
        remote(rsend.at[peer], rrecv.at[ep], r_sem.at[0], r_sem.at[1], peer, x).start()

    weight_out += far_to_mate(up_w)
    weight_out += second_round(down_w)

    landed(tok.at[pl.ds(0, 15)], t_sem.at[1])
    xd[...] = dot(pd[...], tok[...].reshape(512, CH)).astype(BF).reshape(4, 128, CH)
    weight_out += near_to_mate(down_w)
    from_mate(gate_w)
    from_mate(up_w)
    for core in range(2):
        pre_gate = along(xd[0], gbuf[core, 0])
        pre_up = along(xd[0], ubuf[core, 0])
        for q in range(1, 4):
            pre_gate += along(xd[q], gbuf[core, q])
            pre_up += along(xd[q], ubuf[core, q])
        hden[core] = (silu(pre_gate) * pre_up).astype(BF)

    def dense_half(half):
        pair = [
            dot(hden[0], dbuf[0, quarters[n]]) + dot(hden[1], dbuf[1, quarters[n]])
            for n in (2 * half, 2 * half + 1)
        ]
        for n in range(16):
            dsend[half, n] = jnp.concatenate([part[n * 8 : n * 8 + 8] for part in pair], axis=0).astype(BF)
        drecv[half, p] = dsend[half, p]
        for chip, place in zip(chips, places):
            remote(
                dsend.at[half, place], drecv.at[half, p],
                d_sem.at[2 * half], d_sem.at[2 * half + 1], chip + c, x,
            ).start()

    quarters = (x, left, right, far)
    landed(dbuf.at[1 - c, x], dr_sem.at[6])
    landed(dbuf.at[1 - c, left], dr_sem.at[7])
    dense_half(0)
    weight_out += far_to_mate(down_w)
    landed(dbuf.at[1 - c, right], dr_sem.at[8])
    for piece in range(2):
        landed(dbuf.at[1 - c, far, pl.ds(*PIECES[piece])], dr_sem.at[9 + piece])
    dense_half(1)

    landed(rrecv.at[pl.ds(0, 31)], r_sem.at[1])
    back = rrecv[...].reshape(512, CH)
    moe = share_s[0][:, 0:1] * dot(gk[0], back) + share_s[1][:, 0:1] * dot(gk[1], back)
    msend[...] = moe.astype(BF).reshape(4, 32, CH)
    mrecv[x] = msend[x]
    moe_out = []
    for d in (2, 1, 3):
        to = (x + d) % 4
        moe_out.append(remote(msend.at[to], mrecv.at[x], m_sem.at[0], m_sem.at[1], ep, to))
        moe_out[-1].start()

    for half in range(2):
        landed(drecv.at[half, pl.ds(0, 15)], d_sem.at[2 * half + 1])
        total = drecv[half, 0].astype(F32)
        for n in range(1, 16):
            total += drecv[half, n].astype(F32)
        dsum[quarters[2 * half]] = total[0:8]
        dsum[quarters[2 * half + 1]] = total[8:16]
    dense = dsum[...].reshape(32, CH)
    landed(mrecv.at[pl.ds(0, 3)], m_sem.at[1])
    ffn = mrecv[0].astype(F32) + mrecv[1].astype(F32) + mrecv[2].astype(F32) + mrecv[3].astype(F32)
    ffn += mixg_s[:, 0:1] * dense
    scale_ffn = lax.rsqrt(row_total(ffn * ffn) / 2048.0 + EPS)
    fsend[...] = (resid_s[...] + gain(3) * ffn * scale_ffn).reshape(4, 8, CH)
    frecv[x] = fsend[x]
    last_out = []
    for d in (2, 1, 3):
        to = (x + d) % 4
        last_out.append(remote(fsend.at[to], frecv.at[x], f_sem.at[0], f_sem.at[1], ep, to))
        last_out[-1].start()

    for copy in weight_out:
        copy.wait_send()
    landed(bsend.at[pl.ds(0, 3)], b_sem.at[0])
    landed(nall.at[pl.ds(0, 3)], n_sem.at[0])
    landed(tok.at[pl.ds(0, 15)], t_sem.at[0])
    landed(osend.at[pl.ds(0, 31)], o_sem.at[0])
    landed(rsend.at[pl.ds(0, 31)], r_sem.at[0])
    landed(dsend.at[0, pl.ds(0, 15)], d_sem.at[0])
    landed(dsend.at[1, pl.ds(0, 15)], d_sem.at[2])
    landed(msend.at[pl.ds(0, 3)], m_sem.at[0])
    landed(frecv.at[pl.ds(0, 3)], f_sem.at[1])
    out[...] = frecv[...].reshape(32, CH).astype(BF)
    landed(fsend.at[pl.ds(0, 3)], f_sem.at[0])


def whole(*arrays):
    V = pltpu.VMEM
    dma = pltpu.SemaphoreType.DMA
    vm = pl.BlockSpec(memory_space=pltpu.VMEM)
    hb = pl.BlockSpec(memory_space=pltpu.HBM)
    return pl.pallas_call(
        whole_kernel,
        out_shape=(
            V((32, CH), BF), V((32, 2, 128, 128), F32), V((32, 2, 128), F32), V((2, 32), F32),
        ),
        in_specs=[hb] * len(arrays),
        out_specs=(vm,) * 4,
        scratch_shapes=[
            V((32, 2048), BF), V((4, 2048), F32), V((1, 2048), F32), V((2, 32), I32), V((2, 32), F32),
            V((8, 2048), BF), V((8, 2048), BF), V((1, 8), F32), V((2, 32), F32), V((32, 2, 128), F32),
            V((2048, 256), BF), V((2048, 256), BF), V((2048, 256), BF), V((2048, 256), BF),
            V((256, 2048), BF), V((64, 128, 128), F32), V((2, 32, 128), F32),
            V((4, 512, 896), BF), V((4, 512, 896), BF), V((896, 2048), BF),
            V((2, 4, 176, 512), BF), V((2, 4, 176, 512), BF), V((2, 4, 176, 512), BF),
            V((4, 32, CH), BF), V((4, 32, CH), BF), V((4, 32, CH), F32), V((4, 32, CH), BF),
            V((16, 32, CH), BF),
            V((32, 16, CH), BF), V((32, 16, CH), BF), V((32, 16, CH), BF), V((32, 16, CH), BF),
            V((2, 16, 16, CH), BF), V((2, 16, 16, CH), BF), V((4, 8, CH), F32),
            V((4, 32, CH), BF), V((4, 32, CH), BF), V((4, 8, CH), F32), V((4, 8, CH), F32),
            V((512, 512), BF), V((512, 512), BF), V((512, 512), BF), V((512, 128), BF),
            V((2, 128, 512), BF), V((4, 128, CH), BF), V((4, 128, CH), BF),
            V((512, CH), BF), V((128, 896), BF), V((2, 128, 176), BF),
            V((32, CH), F32), V((32, 128), F32), V((2, 128, 128), F32),
            dma((23,)), dma((2,)), dma((2,)), dma((2,)), dma((2,)), dma((2,)), dma((4,)),
            dma((2,)), dma((2,)),
            dma((11,)), dma((11,)), dma((11,)), dma((11,)), dma((11,)), dma((11,)),
        ],
        compiler_params=pltpu.CompilerParams(
            collective_id=0, has_side_effects=True, vmem_limit_bytes=44 * 1024 * 1024
        ),
        name="whole",
    )(*(pltpu.with_memory_space_constraint(a, pltpu.HBM) for a in arrays))


def memory_kernel(matrix, norm, top, last, matrix_h, norm_h, top_h, last_h, sem):
    stores = [
        pltpu.make_async_copy(matrix.at[pl.ds(n * 4, 4)], matrix_h.at[pl.ds(n * 4, 4)], sem.at[n])
        for n in range(8)
    ]
    for n, (src, dst) in enumerate(((norm, norm_h), (top, top_h), (last, last_h))):
        stores.append(pltpu.make_async_copy(src, dst, sem.at[8 + n]))
    for store in stores:
        store.start()
    for store in stores:
        store.wait()


def memory(matrix, norm, top, last):
    arrays = (matrix, norm, top, last)
    return pl.pallas_call(
        memory_kernel,
        out_shape=tuple(pltpu.HBM(a.shape, a.dtype) for a in arrays),
        in_specs=[pl.BlockSpec(memory_space=pltpu.VMEM)] * 4,
        out_specs=(pl.BlockSpec(memory_space=pltpu.HBM),) * 4,
        scratch_shapes=[pltpu.SemaphoreType.DMA((11,))],
        compiler_params=pltpu.CompilerParams(vmem_limit_bytes=16 * 1024 * 1024),
        name="memory",
    )(*arrays)


def local(
    hidden,
    norm_gains,
    w_query,
    w_key,
    w_value,
    w_outgate,
    w_input_gate,
    w_forget_gate,
    forget_bias,
    w_mix_out,
    state_matrix,
    state_norm,
    state_max,
    routes,
    route_scores,
    expert_gate,
    expert_up,
    expert_down,
    dense_gate,
    dense_up,
    dense_down,
    dense_mix,
):
    new_hidden, matrix, norm, top = whole(
        hidden, norm_gains, dense_mix.reshape(1, -1), routes.T, route_scores.T,
        w_input_gate.T, w_forget_gate.T, forget_bias.reshape(1, -1), state_max.T, state_norm,
        w_query, w_key, w_value, w_outgate, w_mix_out, state_matrix.reshape(64, 128, 128),
        expert_gate.reshape(4, CH, -1), expert_up.reshape(4, CH, -1), expert_down[0],
        dense_gate.T, dense_up.T, dense_down,
    )
    new_matrix, new_norm, new_top, new_hidden = memory(matrix, norm, top, new_hidden)
    return (new_hidden, new_matrix, new_norm, new_top.T)


def solution(mesh):
    placed = (
        P("ep", None),
        P(),
        P(None, "tp"),
        P(None, "tp"),
        P(None, "tp"),
        P(None, "tp"),
        P(),
        P(),
        P(),
        P("tp", None),
        P("ep", "tp", None, None),
        P("ep", "tp", None),
        P("ep", "tp"),
        P("ep", None),
        P("ep", None),
        P("ep", None, "tp"),
        P("ep", None, "tp"),
        P("ep", "tp", None),
        P("tp", "ep"),
        P("tp", "ep"),
        P("ep", "tp"),
        P(),
    )
    return jax.shard_map(
        local,
        mesh=mesh,
        in_specs=placed,
        out_specs=(P("ep", "tp"), P("ep", "tp", None, None), P("ep", "tp", None), P("ep", "tp")),
        check_vma=False,
    )
```
